32 devices in a mesh: sp: 4 (over y, x), tp: 8 (over z, core).
Axes of the slice: x: 2, y: 2, z: 4, core: 2. Of those that a mesh axis runs over, the one named last changes fastest.
Arguments:
- skip_stream_entry: bfloat16 [2048, 2048], P(('sp', 'tp')), may hold values from -6 to 6
- result_switch_mapped: bfloat16 [2048, 4096], P('sp', 'tp'), may hold values from -6 to 6
- channel_feed_mapped: bfloat16 [2048, 4096], P('sp', 'tp'), may hold values from -6 to 6
- write_coefficient_mapped: bfloat16 [2048, 2048], P('sp', 'tp'), may hold values from -6 to 6
- emission_coefficient_mapped: bfloat16 [2048, 2048], P('sp', 'tp'), may hold values from -6 to 6
- channel_feed_taps: bfloat16 [5, 4096], P(None, 'tp'), may hold values from -2.5 to 2.5
- write_coefficient_taps: bfloat16 [5, 2048], P(None, 'tp'), may hold values from -2.5 to 2.5
- emission_coefficient_taps: bfloat16 [5, 2048], P(None, 'tp'), may hold values from -2.5 to 2.5
- raw_increments: bfloat16 [2, 64, 2048], P(None, 'tp', 'sp'), may hold values from -6 to 6
- channel_log_fade_speed: float32 [2, 64], P(None, 'tp'), may hold values from -20 to 0
- extra_log_fade: float32 [2, 64, 2048], P(None, 'tp', 'sp'), may hold values from -1 to 0
- cluster_scaling_factor: float32 [4096], P('tp'), may hold values from 0.1 to 1.9
- blend_result_matrix: bfloat16 [4096, 2048], P('tp'), may hold values from -0.09375 to 0.09375
- routing_scaling_factor: float32 [2048], replicated, may hold values from 0.1 to 1.9
- specialist_switch_matrix: bfloat16 [8, 2048, 4096], P('sp', None, 'tp'), may hold values from -0.125 to 0.125
- specialist_widen_matrix: bfloat16 [8, 2048, 4096], P('sp', None, 'tp'), may hold values from -0.125 to 0.125
- specialist_contract_matrix: bfloat16 [8, 4096, 2048], P('sp', 'tp'), may hold values from -0.1875 to 0.1875
- picked_specialists: int32 [2048, 2], P(('sp', 'tp')), may hold values from 0 to 7, all different within a row; in each aligned block of 64 rows (0 to 63, 64 to 127, ...) at most 24 rows name the same one
- router_affinities: float32 [2048, 2], P(('sp', 'tp')), may hold values from 0.1 to 1
Outputs:
- result: bfloat16 [2048, 2048], P(('sp', 'tp'))
The draws below stay inside these ranges and needn't reach their ends.
Inputs may be any that keep to these rules, and one draw needn't show every extreme that they name: `picked_specialists`: each row names 2 different experts. Within the rows of one device (aligned blocks of 64 rows) no expert is named more than 24 times, a bound that some block reaches.
All inputs are finite; a program needn't handle non-finite values.
Results may differ from the reference program's by a relative error of at most 0.02.
Values may be sent and summed in bfloat16 or wider, within the bound.
No kernel may reach another device: no remote copies, remote signals or barrier semaphores. Data moves between devices by JAX's collectives and lax.ppermute only.
A program may use at most 64 MiB of HBM per device.

```python
import math
import jax
import jax.numpy as jnp
import numpy as np
from jax import lax

WIDTH = 2048
HEADS = 64
HEAD_DIM = 64
GROUPS = 16
STATE = 128
EXPERT_FF = 4096
CONV_W = 5
BLOCK = 128
TOP = 2
SEQ_DEV = 512
INNER = 4096
SERIES_ITEMS = 2048
ROWS_DEV = 64
EXPERTS = 8
CAPACITY = 24
N_SP = 4
N_TP = 8


def draw_raw_increments(key, part):
    first_key, second_key = jax.random.split(key)
    noise = 0.7 * jax.random.normal(second_key, (2, HEADS, SERIES_ITEMS), jnp.float32)
    shifts = jax.random.uniform(first_key, (2, HEADS, SERIES_ITEMS // SEQ_DEV), jnp.float32, -1.5, 1.0)
    return (noise + jnp.repeat(shifts, SEQ_DEV, axis=2)).astype(jnp.bfloat16)


def draw_channel_log_fade_speed(key, part):
    coin_key, slow_key, fast_key = jax.random.split(key, 3)
    share = 0.5
    slow = jnp.log(jax.random.uniform(slow_key, (2, HEADS), jnp.float32, 0.1, 0.4) / SERIES_ITEMS)
    fast = jnp.log(jax.random.uniform(fast_key, (2, HEADS), jnp.float32, 0.05, 0.12))
    return jnp.where(jax.random.uniform(coin_key, (2, HEADS), jnp.float32) < share, slow, fast)


def draw_extra_log_fade(key, part):
    place_key, depth_key = jax.random.split(key)
    third = SERIES_ITEMS // 3
    offsets = jnp.arange(3, dtype=jnp.int32) * third
    places = offsets[None, None, :] + jax.random.randint(place_key, (2, HEADS, 3), 0, third, dtype=jnp.int32)
    depths = jnp.log(jax.random.uniform(depth_key, (2, HEADS, 3), jnp.float32, 0.5, 0.8))
    positions = jnp.arange(SERIES_ITEMS, dtype=jnp.int32)
    landed = positions[None, None, None, :] == places[..., None]
    return jnp.sum(jnp.where(landed, depths[..., None], 0.0), axis=2)


def level_of(rng, dims, cuts, least, largest):
    level, own = 1.0, jax.random.fold_in(rng, 6)
    for position, blocks in cuts:
        heights = jnp.exp(jax.random.uniform(jax.random.fold_in(own, position), (blocks,), jnp.float32, least / len(cuts), largest / len(cuts)))
        level = level * jnp.repeat(heights, dims[position] // blocks).reshape([-1 if axis == position else 1 for axis in range(len(dims))])
    return level


def shared_out(stream_key, own, number, rows, number_of, top, bound, skew):
    order = jax.random.permutation(stream_key, number_of)
    heavy_load, common = load_shares(number_of, rows * top, bound, skew, True), load_shares(number_of, rows * top, bound, skew, False)
    places = jnp.arange(number_of)

    def named(lengths, offset_by):
        used = int((lengths > 0).sum())
        fixed = max(1, used // 4)
        moved = fixed + (places - fixed + offset_by * (used - fixed)) % max(1, number_of - fixed)
        return jnp.zeros((number_of,), jnp.int32).at[order[jnp.where(places < fixed, places, moved)]].set(jnp.asarray(lengths, jnp.int32))

    lengths = jnp.where(number % 4 == 0, named(heavy_load, number // 4), named(common, number - number // 4 - 1))
    mixed = jax.random.permutation(jax.random.fold_in(own, 3), number_of)
    source_of, sink = mixed[0:number_of // 2 * 2:2], mixed[1:number_of // 2 * 2:2]
    room = jnp.minimum(lengths[source_of] - 1, bound - lengths[sink]) // 2
    room = jnp.where((source_of == order[0]) | (sink == order[0]) | (lengths[sink] == 0), 0, jnp.maximum(room, 0))
    moved = jax.random.randint(jax.random.fold_in(own, 4), (number_of // 2,), 0, 1 << 20) % (room + 1)
    lengths = lengths.at[source_of].add(-moved).at[sink].add(moved)
    members = jnp.searchsorted(jnp.cumsum(lengths), jnp.arange(rows * top), side="right").astype(jnp.int32)
    table = members.reshape(top, rows).T
    table = table[jax.random.permutation(jax.random.fold_in(own, 1), rows)]
    offset_by = jax.random.randint(jax.random.fold_in(own, 2), (rows, 1), 0, top)
    return jnp.take_along_axis(table, (jnp.arange(top)[None, :] + offset_by) % top, axis=1)


def load_shares(number_of, total, most, lean, full):
    weights = [(1 << 20) // math.isqrt(rank ** lean) + 1 for rank in range(1, number_of + 1)]
    largest = most if full else min(most, max(-(-total // number_of), total * weights[0] // sum(weights)))
    least = 1 if total - largest >= number_of - 1 else 0
    holding, spare = [largest] + [least] * (number_of - 1), total - largest - least * (number_of - 1)
    while spare > 0:
        free = [i for i in range(1, number_of) if holding[i] < largest] or [i for i in range(1, number_of) if holding[i] < most]
        whole, left = sum([weights[i] for i in free]), spare
        for i in free:
            addition = min(most - holding[i], max(1, left * weights[i] // whole), spare)
            holding[i] = holding[i] + addition
            spare = spare - addition
    return np.array(holding)


def scatter_about(rng, shape, scale, bound, cuts=(), kind=jnp.bfloat16):
    entries = scale * jax.random.normal(rng, shape, jnp.float32)
    if cuts:
        entries = entries * level_of(rng, shape, cuts, -0.22, 0.18)
    return jnp.clip(entries, -bound, bound).astype(kind)


def setup_inputs(seed: int = 0) -> dict:
    splits = jax.random.split(jax.random.key(seed), 20)
    skip_stream_entry = scatter_about(splits[0], (SERIES_ITEMS, WIDTH), 1.0, 6.0, ((0, 32),))
    result_switch_mapped = scatter_about(splits[1], (SERIES_ITEMS, INNER), 1.0, 6.0, ((0, 4), (1, 8)))
    channel_feed_mapped = scatter_about(splits[2], (SERIES_ITEMS, INNER), 1.0, 6.0, ((0, 4), (1, 8)))
    write_coefficient_mapped = scatter_about(splits[3], (SERIES_ITEMS, GROUPS * STATE), 1.0, 6.0, ((0, 4), (1, 8)))
    emission_coefficient_mapped = scatter_about(splits[4], (SERIES_ITEMS, GROUPS * STATE), 1.0, 6.0, ((0, 4), (1, 8)))
    channel_feed_taps = scatter_about(splits[5], (CONV_W, INNER), CONV_W ** -0.5, 2.5, ((1, 8),))
    write_coefficient_taps = scatter_about(splits[6], (CONV_W, GROUPS * STATE), CONV_W ** -0.5, 2.5, ((1, 8),))
    emission_coefficient_taps = scatter_about(splits[7], (CONV_W, GROUPS * STATE), CONV_W ** -0.5, 2.5, ((1, 8),))
    raw_increments = draw_raw_increments(jax.random.fold_in(splits[19], 71), 0)
    channel_log_fade_speed = draw_channel_log_fade_speed(jax.random.fold_in(splits[19], 71), 0)
    extra_log_fade = draw_extra_log_fade(jax.random.fold_in(splits[19], 71), 0)
    cluster_scaling_factor = jnp.clip(1.0 + 0.18 * jax.random.normal(splits[11], (INNER,), jnp.float32), 0.1, 1.9)
    blend_result_matrix = scatter_about(splits[12], (INNER, WIDTH), INNER ** -0.5, 0.09375, ((0, 8),))
    routing_scaling_factor = jnp.clip(1.0 + 0.18 * jax.random.normal(splits[13], (WIDTH,), jnp.float32), 0.1, 1.9)
    specialist_switch_matrix = scatter_about(splits[14], (EXPERTS, WIDTH, EXPERT_FF), WIDTH ** -0.5, 0.125, ((0, 4), (2, 8)))
    specialist_widen_matrix = scatter_about(splits[15], (EXPERTS, WIDTH, EXPERT_FF), WIDTH ** -0.5, 0.125, ((0, 4), (2, 8)))
    specialist_contract_matrix = scatter_about(splits[16], (EXPERTS, EXPERT_FF, WIDTH), (EXPERT_FF // 4) ** -0.5, 0.1875, ((0, 4), (1, 8)))
    picked_specialists_keys = jax.random.split(jax.random.fold_in(splits[17], 1), SERIES_ITEMS // ROWS_DEV)
    picked_specialists_turns = jax.random.permutation(jax.random.fold_in(splits[17], 3), SERIES_ITEMS // ROWS_DEV)
    picked_specialists = jax.vmap(lambda own, number: shared_out(jax.random.fold_in(splits[17], 2), own, number, ROWS_DEV, EXPERTS, TOP, CAPACITY, 1))(picked_specialists_keys, picked_specialists_turns).reshape((SERIES_ITEMS, TOP))
    router_affinities = jnp.clip(jnp.exp(math.log(1.0) - 2.3025851 * jax.random.uniform(splits[18], (SERIES_ITEMS, TOP), jnp.float32) ** level_of(splits[18], (SERIES_ITEMS, TOP), ((0, 32),), -0.2, 0.2)), 0.1, 1.0)
    return dict(skip_stream_entry=skip_stream_entry, result_switch_mapped=result_switch_mapped, channel_feed_mapped=channel_feed_mapped, write_coefficient_mapped=write_coefficient_mapped, emission_coefficient_mapped=emission_coefficient_mapped, channel_feed_taps=channel_feed_taps, write_coefficient_taps=write_coefficient_taps, emission_coefficient_taps=emission_coefficient_taps, raw_increments=raw_increments, channel_log_fade_speed=channel_log_fade_speed, extra_log_fade=extra_log_fade, cluster_scaling_factor=cluster_scaling_factor, blend_result_matrix=blend_result_matrix, routing_scaling_factor=routing_scaling_factor, specialist_switch_matrix=specialist_switch_matrix, specialist_widen_matrix=specialist_widen_matrix, specialist_contract_matrix=specialist_contract_matrix, picked_specialists=picked_specialists, router_affinities=router_affinities)


EPSILON = 1e-06
HIGHEST_MODE = lax.Precision.HIGHEST

def centred_conv(padded, weights, series_count):
    summed = jnp.zeros((series_count, padded.shape[1]), jnp.float32)
    for offset in range(weights.shape[0]):
        summed = summed + weights[offset].astype(jnp.float32) * padded[offset:offset + series_count].astype(jnp.float32)
    return jax.nn.silu(summed)

def local_sweep(inputs, entry_state, readout_state, log_fade_factor, softplus_increment):
    seq_len = inputs.shape[0]
    blocks = seq_len // BLOCK
    heads_here = log_fade_factor.shape[0]
    groups_here = entry_state.shape[1] // STATE
    per_group = heads_here // groups_here
    values = inputs.reshape(blocks, BLOCK, groups_here, per_group, HEAD_DIM)
    b_blocks = entry_state.reshape(blocks, BLOCK, groups_here, STATE)
    c_blocks = readout_state.reshape(blocks, BLOCK, groups_here, STATE)
    decay_blocks = log_fade_factor.reshape(groups_here, per_group, blocks, BLOCK)
    step_blocks = softplus_increment.reshape(groups_here, per_group, blocks, BLOCK)
    cumulative = jnp.cumsum(decay_blocks, axis=-1)
    group_inner = jnp.einsum('bign,bjgn->gbij', c_blocks, b_blocks, precision=HIGHEST_MODE)
    spread = cumulative[..., :, None] - cumulative[..., None, :]
    lower_tri = jnp.arange(BLOCK)[:, None] >= jnp.arange(BLOCK)[None, :]
    mixing = jnp.exp(jnp.where(lower_tri, spread, -jnp.inf)) * step_blocks[..., None, :] * group_inner[:, None]
    within = jnp.einsum('gkbij,bjgkp->bigkp', mixing, values, precision=HIGHEST_MODE)
    to_end = jnp.exp(cumulative[..., -1:] - cumulative) * step_blocks
    block_states = jnp.einsum('gkbj,bjgkp,bjgn->bgkpn', to_end, values, b_blocks, precision=HIGHEST_MODE)
    block_decay = cumulative[..., -1]

    def advance(carried, pieces):
        state_piece, decay_piece = pieces
        return (carried * jnp.exp(decay_piece)[..., None, None] + state_piece, carried)
    zero_state = jnp.zeros((groups_here, per_group, HEAD_DIM, STATE), jnp.float32)
    final_state, entering = lax.scan(advance, zero_state, (block_states, jnp.moveaxis(block_decay, -1, 0)))
    before = jnp.cumsum(block_decay, axis=-1) - block_decay
    return ((within, entering, cumulative, before, c_blocks), (lax.optimization_barrier(jnp.sum(block_decay, axis=-1)), final_state))

def finish_sweep(parts, carried):
    within, entering, cumulative, before, c_blocks = parts
    entering = entering + carried[None] * jnp.exp(jnp.moveaxis(before, -1, 0))[..., None, None]
    readout = jnp.einsum('bign,bgkpn->bigkp', c_blocks, entering, precision=HIGHEST_MODE)
    readout = readout * jnp.exp(jnp.transpose(cumulative, (2, 3, 0, 1)))[..., None]
    combined = within + readout
    return combined.reshape(combined.shape[0] * combined.shape[1], -1)

def blend_parts_list(channel_feed_bordered, write_coefficient_bordered, emission_coefficient_bordered, channel_feed_taps, write_coefficient_taps, emission_coefficient_taps, raw_increments, channel_log_fade_speed, extra_log_fade, series_count):
    inputs = centred_conv(channel_feed_bordered, channel_feed_taps, series_count)
    entry_state = centred_conv(write_coefficient_bordered, write_coefficient_taps, series_count)
    readout_state = centred_conv(emission_coefficient_bordered, emission_coefficient_taps, series_count)
    softplus_increment = jax.nn.softplus(raw_increments.astype(jnp.float32))
    log_fade_factor = -softplus_increment * jnp.exp(channel_log_fade_speed)[..., None] + extra_log_fade
    onward_pass = local_sweep(inputs, entry_state, readout_state, log_fade_factor[0], softplus_increment[0])
    backward_pass = local_sweep(jnp.flip(inputs, 0), jnp.flip(entry_state, 0), jnp.flip(readout_state, 0), jnp.flip(log_fade_factor[1], -1), jnp.flip(softplus_increment[1], -1))
    return (onward_pass, backward_pass)

def gated_norm(mixed_sum, result_switch_mapped, cluster_scaling_factor):
    gated = mixed_sum * jax.nn.silu(result_switch_mapped.astype(jnp.float32))
    grouped = gated.reshape(gated.shape[0], -1, INNER // GROUPS)
    normalized = grouped * lax.rsqrt(lax.optimization_barrier(jnp.mean(grouped * grouped, axis=-1, keepdims=True)) + EPSILON)
    return (normalized.reshape(gated.shape) * cluster_scaling_factor).astype(jnp.bfloat16)

def rms_scale(stream, gain):
    values = stream.astype(jnp.float32)
    return (values * lax.rsqrt(lax.optimization_barrier(jnp.mean(values * values, axis=-1, keepdims=True)) + EPSILON) * gain).astype(jnp.bfloat16)

def reference(skip_stream_entry, result_switch_mapped, channel_feed_mapped, write_coefficient_mapped, emission_coefficient_mapped, channel_feed_taps, write_coefficient_taps, emission_coefficient_taps, raw_increments, channel_log_fade_speed, extra_log_fade, cluster_scaling_factor, blend_result_matrix, routing_scaling_factor, specialist_switch_matrix, specialist_widen_matrix, specialist_contract_matrix, picked_specialists, router_affinities):
    rim_width = CONV_W // 2
    filter_border_width = ((rim_width, rim_width), (0, 0))
    onward_pass, backward_pass = blend_parts_list(jnp.pad(channel_feed_mapped, filter_border_width), jnp.pad(write_coefficient_mapped, filter_border_width), jnp.pad(emission_coefficient_mapped, filter_border_width), channel_feed_taps, write_coefficient_taps, emission_coefficient_taps, raw_increments, channel_log_fade_speed, extra_log_fade, SERIES_ITEMS)
    zero_carry = jnp.zeros_like(onward_pass[1][1])
    mixed_sum = finish_sweep(onward_pass[0], zero_carry) + jnp.flip(finish_sweep(backward_pass[0], zero_carry), 0)
    mixed_rows = gated_norm(mixed_sum, result_switch_mapped, cluster_scaling_factor)
    slice_width = INNER // N_TP

    def add_slice(summed, slice_index):
        columns = lax.dynamic_slice_in_dim(mixed_rows, slice_index * slice_width, slice_width, 1)
        weights = lax.dynamic_slice_in_dim(blend_result_matrix, slice_index * slice_width, slice_width, 0)
        partial_sum = jnp.dot(columns, weights, preferred_element_type=jnp.float32).astype(jnp.bfloat16)
        partial_sum = lax.optimization_barrier(partial_sum)
        return (summed + partial_sum.astype(jnp.float32), slice_index)
    projected = lax.scan(add_slice, jnp.zeros((SERIES_ITEMS, WIDTH), jnp.float32), jnp.arange(N_TP, dtype=jnp.int32))[0]
    after_mixer = (skip_stream_entry.astype(jnp.float32) + projected).astype(jnp.bfloat16)
    normed = rms_scale(after_mixer, routing_scaling_factor)
    row_count = SERIES_ITEMS * TOP
    flat_routes = picked_specialists.reshape(row_count)
    owner = jnp.arange(row_count, dtype=jnp.int32) // TOP
    limit = N_SP * N_TP * CAPACITY
    ff_slice = EXPERT_FF // N_TP

    def one_expert(outputs, expert):
        chosen = flat_routes == expert
        chosen_rank = jnp.cumsum(chosen.astype(jnp.int32)) - 1
        target = jnp.where(chosen, chosen_rank, limit)
        member = jnp.zeros((limit,), jnp.int32).at[target].set(jnp.arange(row_count, dtype=jnp.int32), mode='drop')
        filled = jnp.zeros((limit,), jnp.int32).at[target].set(1, mode='drop')
        picked = normed[owner[member]]
        gate_part = jnp.dot(picked, specialist_switch_matrix[expert], preferred_element_type=jnp.float32)
        up_part = jnp.dot(picked, specialist_widen_matrix[expert], preferred_element_type=jnp.float32)
        hidden = (jax.nn.silu(gate_part) * up_part).astype(jnp.bfloat16)
        pieces = jnp.einsum('rsf,sfd->rsd', hidden.reshape(limit, N_TP, ff_slice).astype(jnp.float32), specialist_contract_matrix[expert].reshape(N_TP, ff_slice, WIDTH).astype(jnp.float32))
        pieces = lax.optimization_barrier(pieces.astype(jnp.bfloat16))
        expert_out = lax.optimization_barrier(jnp.sum(pieces.astype(jnp.float32), axis=1)).astype(jnp.bfloat16)
        destination = jnp.where(filled > 0, member, row_count)
        return (outputs.at[destination].set(expert_out, mode='drop'), expert)
    assigned = lax.scan(one_expert, jnp.zeros((row_count, WIDTH), jnp.bfloat16), jnp.arange(EXPERTS, dtype=jnp.int32))[0]
    weights = router_affinities / lax.optimization_barrier(jnp.sum(router_affinities, axis=-1, keepdims=True))
    mixture = lax.optimization_barrier(jnp.sum(weights[..., None] * assigned.reshape(SERIES_ITEMS, TOP, WIDTH).astype(jnp.float32), axis=1))
    return (after_mixer.astype(jnp.float32) + mixture).astype(jnp.bfloat16)
```

```python
import functools
import math

import jax
import jax.numpy as jnp
from jax import lax
from jax.experimental import pallas as pl
from jax.experimental.pallas import tpu as pltpu
from jax.sharding import PartitionSpec as P

HEAD_DIM = 64
STATE = 128
TOP = 2
TILE = 128
PAD = 8
EXTRA = 16

EPSILON = 1e-06
LOG2E = math.log2(math.e)
F32, BF16 = jnp.float32, jnp.bfloat16


def silu(v):
    return v / (1.0 + jnp.exp(-v))


def over_heads(columns, first, count):
    rows = columns.shape[0]
    lane = lax.broadcasted_iota(jnp.int32, (rows, 2 * HEAD_DIM), 1)
    pairs = []
    for h in range(0, count, 2):
        a = jnp.broadcast_to(columns[:, first + h : first + h + 1], lane.shape)
        b = jnp.broadcast_to(columns[:, first + h + 1 : first + h + 2], lane.shape)
        pairs.append(jnp.where(lane < HEAD_DIM, a, b))
    return jnp.concatenate(pairs, axis=1)


def prepare_kernel(
    x_ref, b_ref, c_ref, low_ref, high_ref, tx_ref, tb_ref, tc_ref, raw_ref, speed_ref, fade_ref,
    xc_ref, bc_ref, cc_ref, rows_ref, cols_ref, *rest, axis,
):
    *msg_refs, pad_ref = rest
    steps = x_ref.shape[0]
    heads = raw_ref.shape[1]
    groups = b_ref.shape[1] // STATE
    per_group = heads // groups
    wide = per_group * HEAD_DIM
    here = lax.axis_index(axis)

    lane = lax.broadcasted_iota(jnp.int32, (heads, steps), 1)
    eye = lax.broadcasted_iota(jnp.int32, (heads, heads), 0) == lax.broadcasted_iota(
        jnp.int32, (heads, heads), 1
    )
    sums, weights, totals = [], [], []
    for d in range(2):
        raw = raw_ref[d].astype(F32)
        step = jnp.maximum(raw, 0.0) + jnp.log1p(jnp.exp(-jnp.abs(raw)))
        speed = jnp.sum(
            jnp.where(eye, jnp.exp(speed_ref[d : d + 1, :]), 0.0), axis=1, keepdims=True
        )
        run = -step * speed + fade_ref[d]
        shift = 1
        while shift < steps:
            if d == 0:
                run = run + jnp.where(lane >= shift, pltpu.roll(run, shift, 1), 0.0)
            else:
                run = run + jnp.where(lane < steps - shift, pltpu.roll(run, steps - shift, 1), 0.0)
            shift *= 2
        total = run[:, steps - 1 : steps] if d == 0 else run[:, 0:1]
        totals.append(total)
        sums.append(run * LOG2E)
        weights.append(jnp.exp(total - run) * step)
        rows_ref[d] = run * LOG2E - jnp.log(step) * LOG2E
    stacked = jnp.concatenate(
        sums + weights + [jnp.zeros((STATE - 4 * heads, steps), F32)], axis=0
    )
    cols = stacked.T
    cols_ref[...] = cols

    def conv(ref, taps_ref, at, start):
        pad_ref[PAD - 2 : PAD] = low_ref[:, at + start : at + start + TILE].astype(F32)
        pad_ref[PAD : PAD + steps] = ref[:, start : start + TILE].astype(F32)
        pad_ref[PAD + steps : PAD + steps + 2] = high_ref[
            :, at + start : at + start + TILE
        ].astype(F32)
        taps = taps_ref[:, start : start + TILE].astype(F32)
        total = taps[0:1] * pad_ref[PAD - 2 : PAD - 2 + steps]
        for j in range(1, taps.shape[0]):
            total = total + taps[j : j + 1] * pad_ref[PAD - 2 + j : PAD - 2 + j + steps]
        return silu(total)

    at = 0
    for ref, taps_ref, out_ref in (
        (x_ref, tx_ref, xc_ref), (b_ref, tb_ref, bc_ref), (c_ref, tc_ref, cc_ref),
    ):
        for start in range(0, ref.shape[1], TILE):
            out_ref[:, start : start + TILE] = conv(ref, taps_ref, at, start).astype(BF16)
        at += ref.shape[1]

    row = lax.broadcasted_iota(jnp.int32, (EXTRA, wide), 0)
    own = lax.broadcasted_iota(jnp.int32, (per_group, wide), 0) == (
        lax.broadcasted_iota(jnp.int32, (per_group, wide), 1) // HEAD_DIM
    )
    for g in range(groups):
        turned = bc_ref[:, g * STATE : (g + 1) * STATE].astype(F32).T.astype(BF16)
        xg = xc_ref[:, g * wide : (g + 1) * wide].astype(F32)
        both = []
        for d in range(2):
            weight = over_heads(cols, (2 + d) * heads + g * per_group, per_group)
            state = jnp.dot(turned, (xg * weight).astype(BF16), preferred_element_type=F32)
            total = jnp.sum(
                jnp.where(own, totals[d][g * per_group : (g + 1) * per_group], 0.0),
                axis=0, keepdims=True,
            )
            upper = total.astype(BF16).astype(F32)
            extra = jnp.where(row == 0, upper, jnp.where(row == 1, total - upper, 0.0))
            both.append((state, extra))
        for k, msg_ref in enumerate(msg_refs, 1):
            onward = jnp.where((here ^ k) > here, 1.0, 0.0).astype(F32)
            (sf, ef), (sb, eb) = both
            msg_ref[g, 0:STATE, :] = (sf * onward + sb * (1.0 - onward)).astype(BF16)
            msg_ref[g, STATE : STATE + EXTRA, :] = (ef * onward + eb * (1.0 - onward)).astype(BF16)


def local_kernel(xc_ref, bc_ref, cc_ref, rows_ref, cols_ref, y_ref):
    steps = xc_ref.shape[0]
    heads = rows_ref.shape[1]
    groups = bc_ref.shape[1] // STATE
    per_group = heads // groups
    tiles = steps // TILE
    i_at = lax.broadcasted_iota(jnp.int32, (TILE, TILE), 0)
    j_at = lax.broadcasted_iota(jnp.int32, (TILE, TILE), 1)
    for g in range(groups):
        for i in range(tiles):
            span = slice(i * TILE, (i + 1) * TILE)
            inner = lax.dot_general(
                cc_ref[span, g * STATE : (g + 1) * STATE],
                bc_ref[:, g * STATE : (g + 1) * STATE],
                (((1,), (1,)), ((), ())),
                preferred_element_type=F32,
            )
            for pair in range(per_group // 2):
                halves = []
                at = (g * per_group + 2 * pair) * HEAD_DIM
                for h in (g * per_group + 2 * pair, g * per_group + 2 * pair + 1):
                    here_f = jnp.broadcast_to(cols_ref[span, h : h + 1], (TILE, TILE))
                    here_b = jnp.broadcast_to(cols_ref[span, heads + h : heads + h + 1], (TILE, TILE))
                    parts = []
                    for j in range(tiles):
                        js = slice(j * TILE, (j + 1) * TILE)
                        if j <= i:
                            mix = jnp.exp2(here_f - rows_ref[0, h : h + 1, js])
                            if j == i:
                                mix = jnp.where(i_at >= j_at, mix, 0.0) + jnp.where(
                                    i_at <= j_at, jnp.exp2(here_b - rows_ref[1, h : h + 1, js]), 0.0
                                )
                        else:
                            mix = jnp.exp2(here_b - rows_ref[1, h : h + 1, js])
                        parts.append((mix * inner[:, js]).astype(BF16))
                    halves.append(
                        jnp.dot(
                            jnp.concatenate(parts, axis=1),
                            xc_ref[:, at : at + 2 * HEAD_DIM],
                            preferred_element_type=F32,
                        )
                    )
                y_ref[span, at : at + 2 * HEAD_DIM] = jnp.where(j_at < HEAD_DIM, *halves)


def finish_kernel(y_ref, cc_ref, cols_ref, switch_ref, gain_ref, *rest, axis):
    *msg_refs, out_ref, carry_ref = rest
    steps, channels = y_ref.shape
    groups = cc_ref.shape[1] // STATE
    wide = channels // groups
    per_group = wide // HEAD_DIM
    heads = groups * per_group
    here = lax.axis_index(axis)
    peers = [here ^ k for k in range(1, len(msg_refs) + 1)]

    def flag(condition):
        return jnp.where(condition, 1.0, 0.0).astype(F32)

    for g in range(groups):
        totals = [
            ref[g, STATE : STATE + 1, :].astype(F32) + ref[g, STATE + 1 : STATE + 2, :].astype(F32)
            for ref in msg_refs
        ]
        for d in range(2):
            carry = jnp.zeros((STATE, wide), F32)
            for k, ref in enumerate(msg_refs):
                between = jnp.zeros((1, wide), F32)
                for other in range(len(msg_refs)):
                    if other != k:
                        if d == 0:
                            inside = (peers[k] < peers[other]) & (peers[other] < here)
                        else:
                            inside = (peers[k] > peers[other]) & (peers[other] > here)
                        between = between + flag(inside) * totals[other]
                mine = flag(peers[k] < here if d == 0 else peers[k] > here)
                carry = carry + ref[g, 0:STATE, :].astype(F32) * (mine * jnp.exp(between))
            carry_ref[d] = carry.astype(BF16)
        for i in range(steps // TILE):
            span = slice(i * TILE, (i + 1) * TILE)
            lanes = slice(g * wide, (g + 1) * wide)
            cols = jnp.exp2(cols_ref[span, :])
            cc = cc_ref[span, g * STATE : (g + 1) * STATE]
            y = y_ref[span, lanes]
            for d in range(2):
                y = y + over_heads(cols, d * heads + g * per_group, per_group) * jnp.dot(
                    cc, carry_ref[d], preferred_element_type=F32
                )
            gated = y * silu(switch_ref[span, lanes].astype(F32))
            mean = jnp.sum(gated * gated, axis=1, keepdims=True) * (1.0 / wide)
            out_ref[span, lanes] = (
                gated * lax.rsqrt(mean + EPSILON) * gain_ref[:, lanes]
            ).astype(BF16)


def vmem(count):
    return [pl.BlockSpec(memory_space=pltpu.VMEM) for _ in range(count)]


def mixer(x, b, c, tx, tb, tc, raw, speed, fade, switch, gain):
    steps, channels = x.shape
    heads = raw.shape[1]
    groups = b.shape[1] // STATE
    wide = channels // groups
    rim = tx.shape[0] // 2
    count = lax.axis_size("sp")
    first = jnp.concatenate([x[:rim], b[:rim], c[:rim]], axis=1)
    last = jnp.concatenate([x[-rim:], b[-rim:], c[-rim:]], axis=1)
    low = lax.ppermute(last, "sp", [(i, i + 1) for i in range(count - 1)])
    high = lax.ppermute(first, "sp", [(i + 1, i) for i in range(count - 1)])
    message = jax.ShapeDtypeStruct((groups, STATE + EXTRA, wide), BF16)
    xc, bc, cc, rows, cols, *sends = pl.pallas_call(
        functools.partial(prepare_kernel, axis="sp"),
        out_shape=[
            jax.ShapeDtypeStruct(x.shape, BF16),
            jax.ShapeDtypeStruct(b.shape, BF16),
            jax.ShapeDtypeStruct(c.shape, BF16),
            jax.ShapeDtypeStruct((2, heads, steps), F32),
            jax.ShapeDtypeStruct((steps, STATE), F32),
        ]
        + [message] * (count - 1),
        in_specs=vmem(11),
        out_specs=vmem(5 + count - 1),
        scratch_shapes=[pltpu.VMEM((steps + 2 * PAD, TILE), F32)],
        name="prepare",
    )(x, b, c, low, high, tx, tb, tc, raw, speed, fade)
    arrived = [
        lax.ppermute(send, "sp", [(i, i ^ k) for i in range(count)])
        for k, send in enumerate(sends, 1)
    ]
    y = pl.pallas_call(
        local_kernel,
        out_shape=jax.ShapeDtypeStruct(x.shape, F32),
        in_specs=vmem(5),
        out_specs=vmem(1)[0],
        cost_estimate=pl.CostEstimate(
            flops=2 * steps * steps * (channels + groups * STATE) * 4,
            bytes_accessed=8 * steps * channels,
            transcendentals=heads * steps * steps,
        ),
        name="local",
    )(xc, bc, cc, rows, cols)
    return pl.pallas_call(
        functools.partial(finish_kernel, axis="sp"),
        out_shape=jax.ShapeDtypeStruct(x.shape, BF16),
        in_specs=vmem(5 + count - 1),
        out_specs=vmem(1)[0],
        scratch_shapes=[pltpu.VMEM((2, STATE, wide), BF16)],
        name="finish",
    )(y, cc, cols, switch, gain.reshape(1, -1), *arrived)


def rms_scale(stream, gain):
    values = stream.astype(jnp.float32)
    return (
        values * lax.rsqrt(jnp.mean(values * values, axis=-1, keepdims=True) + EPSILON) * gain
    ).astype(jnp.bfloat16)


def per_device(
    skip_stream_entry,
    result_switch_mapped,
    channel_feed_mapped,
    write_coefficient_mapped,
    emission_coefficient_mapped,
    channel_feed_taps,
    write_coefficient_taps,
    emission_coefficient_taps,
    raw_increments,
    channel_log_fade_speed,
    extra_log_fade,
    cluster_scaling_factor,
    blend_result_matrix,
    routing_scaling_factor,
    specialist_switch_matrix,
    specialist_widen_matrix,
    specialist_contract_matrix,
    picked_specialists,
    router_affinities,
):
    mixed_rows = mixer(
        channel_feed_mapped,
        write_coefficient_mapped,
        emission_coefficient_mapped,
        channel_feed_taps,
        write_coefficient_taps,
        emission_coefficient_taps,
        raw_increments,
        channel_log_fade_speed,
        extra_log_fade,
        result_switch_mapped,
        cluster_scaling_factor,
    )
    rows_here = skip_stream_entry.shape[0]
    projected = lax.psum_scatter(
        jnp.dot(mixed_rows, blend_result_matrix, preferred_element_type=jnp.float32).astype(
            jnp.bfloat16
        ),
        "tp",
        scatter_dimension=0,
        tiled=True,
    ).astype(jnp.float32)
    after_mixer = (skip_stream_entry.astype(jnp.float32) + projected).astype(jnp.bfloat16)
    normed = rms_scale(after_mixer, routing_scaling_factor)
    experts_here = specialist_switch_matrix.shape[0]
    expert_count = experts_here * lax.axis_size("sp")
    capacity = max(2, 3 * TOP * rows_here // (2 * expert_count))
    slot_total = capacity * expert_count
    flat_routes = picked_specialists.reshape(-1)
    one_hot = (flat_routes[:, None] == jnp.arange(expert_count, dtype=jnp.int32)[None, :]).astype(
        jnp.int32
    )
    earlier_count = jnp.cumsum(one_hot, axis=0) - one_hot
    slot_rank = jnp.sum(earlier_count * one_hot, axis=1)
    position = slot_rank * expert_count + flat_routes
    slot_match = (position[:, None] == jnp.arange(slot_total, dtype=jnp.int32)[None, :]).astype(
        jnp.bfloat16
    )
    buffer = jnp.einsum(
        "rks,rd->sd",
        slot_match.reshape(rows_here, TOP, slot_total),
        normed,
        preferred_element_type=jnp.float32,
    ).astype(jnp.bfloat16)
    buffer = buffer.reshape(capacity, expert_count, skip_stream_entry.shape[1])
    received = lax.all_to_all(buffer, "sp", split_axis=1, concat_axis=0, tiled=True)
    data_block = lax.all_gather(received, "tp", axis=0, tiled=True)
    gate_part = jnp.einsum(
        "red,edf->ref", data_block, specialist_switch_matrix, preferred_element_type=jnp.float32
    )
    up_part = jnp.einsum(
        "red,edf->ref", data_block, specialist_widen_matrix, preferred_element_type=jnp.float32
    )
    hidden = (jax.nn.silu(gate_part) * up_part).astype(jnp.bfloat16)
    expert_out = lax.psum_scatter(
        jnp.einsum(
            "ref,efd->red", hidden, specialist_contract_matrix, preferred_element_type=jnp.float32
        ).astype(jnp.bfloat16),
        "tp",
        scatter_dimension=0,
        tiled=True,
    )
    returned = lax.all_to_all(expert_out, "sp", split_axis=0, concat_axis=1, tiled=True)
    picked = jnp.dot(
        slot_match, returned.reshape(slot_total, skip_stream_entry.shape[1]), preferred_element_type=jnp.float32
    )
    weights = router_affinities / jnp.sum(router_affinities, axis=-1, keepdims=True)
    mixture = jnp.sum(weights[..., None] * picked.reshape(rows_here, TOP, skip_stream_entry.shape[1]), axis=1)
    return (after_mixer.astype(jnp.float32) + mixture).astype(jnp.bfloat16)


def solution(mesh):
    in_specs = (
        P(("sp", "tp"), None),
        P("sp", "tp"),
        P("sp", "tp"),
        P("sp", "tp"),
        P("sp", "tp"),
        P(None, "tp"),
        P(None, "tp"),
        P(None, "tp"),
        P(None, "tp", "sp"),
        P(None, "tp"),
        P(None, "tp", "sp"),
        P("tp"),
        P("tp", None),
        P(),
        P("sp", None, "tp"),
        P("sp", None, "tp"),
        P("sp", "tp", None),
        P(("sp", "tp"), None),
        P(("sp", "tp"), None),
    )
    out_specs = P(("sp", "tp"), None)
    return jax.shard_map(
        per_device, mesh=mesh, in_specs=in_specs, out_specs=out_specs, check_vma=False
    )
```

```python
import functools
import math

import jax
import jax.numpy as jnp
from jax import lax
from jax.experimental import pallas as pl
from jax.experimental.pallas import tpu as pltpu
from jax.sharding import PartitionSpec as P

HEAD_DIM = 64
STATE = 128
TOP = 2
TILE = 128
PAD = 8
EXTRA = 16

EPSILON = 1e-06
LOG2E = math.log2(math.e)
F32, BF16 = jnp.float32, jnp.bfloat16


CORES = 2


def chip_and_core(axis):
    at = lax.axis_index(axis)
    return at // CORES, at & (CORES - 1)


def silu(v):
    return v / (1.0 + jnp.exp(-v))


def over_heads(columns, first, count):
    rows = columns.shape[0]
    lane = lax.broadcasted_iota(jnp.int32, (rows, 2 * HEAD_DIM), 1)
    pairs = []
    for h in range(0, count, 2):
        a = jnp.broadcast_to(columns[:, first + h : first + h + 1], lane.shape)
        b = jnp.broadcast_to(columns[:, first + h + 1 : first + h + 2], lane.shape)
        pairs.append(jnp.where(lane < HEAD_DIM, a, b))
    return jnp.concatenate(pairs, axis=1)


def prepare_kernel(
    x_ref, b_ref, c_ref, low_ref, high_ref, tx_ref, tb_ref, tc_ref, raw_ref, speed_ref, fade_ref,
    xc_ref, bc_ref, cc_ref, rows_ref, cols_ref, *rest, axis,
):
    *msg_refs, pad_ref = rest
    steps = x_ref.shape[0]
    heads = raw_ref.shape[1]
    groups = b_ref.shape[1] // STATE
    per_group = heads // groups
    wide = per_group * HEAD_DIM
    here = lax.axis_index(axis)

    lane = lax.broadcasted_iota(jnp.int32, (heads, steps), 1)
    eye = lax.broadcasted_iota(jnp.int32, (heads, heads), 0) == lax.broadcasted_iota(
        jnp.int32, (heads, heads), 1
    )
    sums, weights, totals = [], [], []
    for d in range(2):
        raw = raw_ref[d].astype(F32)
        step = jnp.maximum(raw, 0.0) + jnp.log1p(jnp.exp(-jnp.abs(raw)))
        speed = jnp.sum(
            jnp.where(eye, jnp.exp(speed_ref[d : d + 1, :]), 0.0), axis=1, keepdims=True
        )
        run = -step * speed + fade_ref[d]
        shift = 1
        while shift < steps:
            if d == 0:
                run = run + jnp.where(lane >= shift, pltpu.roll(run, shift, 1), 0.0)
            else:
                run = run + jnp.where(lane < steps - shift, pltpu.roll(run, steps - shift, 1), 0.0)
            shift *= 2
        total = run[:, steps - 1 : steps] if d == 0 else run[:, 0:1]
        totals.append(total)
        sums.append(run * LOG2E)
        weights.append(jnp.exp(total - run) * step)
        rows_ref[d] = run * LOG2E - jnp.log(step) * LOG2E
    stacked = jnp.concatenate(
        sums + weights + [jnp.zeros((STATE - 4 * heads, steps), F32)], axis=0
    )
    cols = stacked.T
    cols_ref[...] = cols

    def conv(ref, taps_ref, at, start):
        pad_ref[PAD - 2 : PAD] = low_ref[:, at + start : at + start + TILE].astype(F32)
        pad_ref[PAD : PAD + steps] = ref[:, start : start + TILE].astype(F32)
        pad_ref[PAD + steps : PAD + steps + 2] = high_ref[
            :, at + start : at + start + TILE
        ].astype(F32)
        taps = taps_ref[:, start : start + TILE].astype(F32)
        total = taps[0:1] * pad_ref[PAD - 2 : PAD - 2 + steps]
        for j in range(1, taps.shape[0]):
            total = total + taps[j : j + 1] * pad_ref[PAD - 2 + j : PAD - 2 + j + steps]
        return silu(total)

    at = 0
    for ref, taps_ref, out_ref in (
        (x_ref, tx_ref, xc_ref), (b_ref, tb_ref, bc_ref), (c_ref, tc_ref, cc_ref),
    ):
        for start in range(0, ref.shape[1], TILE):
            out_ref[:, start : start + TILE] = conv(ref, taps_ref, at, start).astype(BF16)
        at += ref.shape[1]

    row = lax.broadcasted_iota(jnp.int32, (EXTRA, wide), 0)
    own = lax.broadcasted_iota(jnp.int32, (per_group, wide), 0) == (
        lax.broadcasted_iota(jnp.int32, (per_group, wide), 1) // HEAD_DIM
    )
    for g in range(groups):
        turned = bc_ref[:, g * STATE : (g + 1) * STATE].astype(F32).T.astype(BF16)
        xg = xc_ref[:, g * wide : (g + 1) * wide].astype(F32)
        both = []
        for d in range(2):
            weight = over_heads(cols, (2 + d) * heads + g * per_group, per_group)
            state = jnp.dot(turned, (xg * weight).astype(BF16), preferred_element_type=F32)
            total = jnp.sum(
                jnp.where(own, totals[d][g * per_group : (g + 1) * per_group], 0.0),
                axis=0, keepdims=True,
            )
            upper = total.astype(BF16).astype(F32)
            extra = jnp.where(row == 0, upper, jnp.where(row == 1, total - upper, 0.0))
            both.append((state, extra))
        for k, msg_ref in enumerate(msg_refs, 1):
            onward = jnp.where((here ^ k) > here, 1.0, 0.0).astype(F32)
            (sf, ef), (sb, eb) = both
            msg_ref[g, 0:STATE, :] = (sf * onward + sb * (1.0 - onward)).astype(BF16)
            msg_ref[g, STATE : STATE + EXTRA, :] = (ef * onward + eb * (1.0 - onward)).astype(BF16)


def local_kernel(xc_ref, bc_ref, cc_ref, rows_ref, cols_ref, y_ref):
    steps = xc_ref.shape[0]
    heads = rows_ref.shape[1]
    groups = bc_ref.shape[1] // STATE
    per_group = heads // groups
    tiles = steps // TILE
    i_at = lax.broadcasted_iota(jnp.int32, (TILE, TILE), 0)
    j_at = lax.broadcasted_iota(jnp.int32, (TILE, TILE), 1)
    for g in range(groups):
        for i in range(tiles):
            span = slice(i * TILE, (i + 1) * TILE)
            inner = lax.dot_general(
                cc_ref[span, g * STATE : (g + 1) * STATE],
                bc_ref[:, g * STATE : (g + 1) * STATE],
                (((1,), (1,)), ((), ())),
                preferred_element_type=F32,
            )
            for pair in range(per_group // 2):
                halves = []
                at = (g * per_group + 2 * pair) * HEAD_DIM
                for h in (g * per_group + 2 * pair, g * per_group + 2 * pair + 1):
                    here_f = jnp.broadcast_to(cols_ref[span, h : h + 1], (TILE, TILE))
                    here_b = jnp.broadcast_to(cols_ref[span, heads + h : heads + h + 1], (TILE, TILE))
                    parts = []
                    for j in range(tiles):
                        js = slice(j * TILE, (j + 1) * TILE)
                        if j <= i:
                            mix = jnp.exp2(here_f - rows_ref[0, h : h + 1, js])
                            if j == i:
                                mix = jnp.where(i_at >= j_at, mix, 0.0) + jnp.where(
                                    i_at <= j_at, jnp.exp2(here_b - rows_ref[1, h : h + 1, js]), 0.0
                                )
                        else:
                            mix = jnp.exp2(here_b - rows_ref[1, h : h + 1, js])
                        parts.append((mix * inner[:, js]).astype(BF16))
                    halves.append(
                        jnp.dot(
                            jnp.concatenate(parts, axis=1),
                            xc_ref[:, at : at + 2 * HEAD_DIM],
                            preferred_element_type=F32,
                        )
                    )
                y_ref[span, at : at + 2 * HEAD_DIM] = jnp.where(j_at < HEAD_DIM, *halves)


def finish_kernel(y_ref, cc_ref, cols_ref, switch_ref, gain_ref, *rest, axis, minor, rows):
    *msg_refs, keep_ref, send_ref, carry_ref = rest
    steps, channels = y_ref.shape
    groups = cc_ref.shape[1] // STATE
    wide = channels // groups
    per_group = wide // HEAD_DIM
    heads = groups * per_group
    here = lax.axis_index(axis)
    chip, core = chip_and_core(minor)
    chips = lax.axis_size(minor) // CORES
    peers = [here ^ k for k in range(1, len(msg_refs) + 1)]

    def flag(condition):
        return jnp.where(condition, 1.0, 0.0).astype(F32)

    for g in range(groups):
        totals = [
            ref[g, STATE : STATE + 1, :].astype(F32) + ref[g, STATE + 1 : STATE + 2, :].astype(F32)
            for ref in msg_refs
        ]
        for d in range(2):
            carry = jnp.zeros((STATE, wide), F32)
            for k, ref in enumerate(msg_refs):
                between = jnp.zeros((1, wide), F32)
                for other in range(len(msg_refs)):
                    if other != k:
                        if d == 0:
                            inside = (peers[k] < peers[other]) & (peers[other] < here)
                        else:
                            inside = (peers[k] > peers[other]) & (peers[other] > here)
                        between = between + flag(inside) * totals[other]
                mine = flag(peers[k] < here if d == 0 else peers[k] > here)
                carry = carry + ref[g, 0:STATE, :].astype(F32) * (mine * jnp.exp(between))
            carry_ref[d] = carry.astype(BF16)
        for i in range(steps // TILE):
            span = slice(i * TILE, (i + 1) * TILE)
            lanes = slice(g * wide, (g + 1) * wide)
            cols = jnp.exp2(cols_ref[span, :])
            cc = cc_ref[span, g * STATE : (g + 1) * STATE]
            y = y_ref[span, lanes]
            for d in range(2):
                y = y + over_heads(cols, d * heads + g * per_group, per_group) * jnp.dot(
                    cc, carry_ref[d], preferred_element_type=F32
                )
            gated = y * silu(switch_ref[span, lanes].astype(F32))
            mean = jnp.sum(gated * gated, axis=1, keepdims=True) * (1.0 / wide)
            mixed = gated * lax.rsqrt(mean + EPSILON) * gain_ref[:, lanes]
            for part in range(TILE // (CORES * rows)):
                block = i * (TILE // (CORES * rows)) + part
                south = mixed[part * CORES * rows : (part * CORES + 1) * rows]
                north = mixed[(part * CORES + 1) * rows : (part + 1) * CORES * rows]
                odd = flag(core == 1)
                at = pl.multiple_of(((block - chip) & (chips - 1)) * rows, rows)
                keep_ref[pl.ds(at, rows), lanes] = (south * (1.0 - odd) + north * odd).astype(BF16)
                send_ref[pl.ds(at, rows), lanes] = (south * odd + north * (1.0 - odd)).astype(BF16)


def vmem(count):
    return [pl.BlockSpec(memory_space=pltpu.VMEM) for _ in range(count)]


def mixer(x, b, c, tx, tb, tc, raw, speed, fade, switch, gain, block_rows):
    steps, channels = x.shape
    heads = raw.shape[1]
    groups = b.shape[1] // STATE
    wide = channels // groups
    rim = tx.shape[0] // 2
    count = lax.axis_size("sp")
    first = jnp.concatenate([x[:rim], b[:rim], c[:rim]], axis=1)
    last = jnp.concatenate([x[-rim:], b[-rim:], c[-rim:]], axis=1)
    low = lax.ppermute(last, "sp", [(i, i + 1) for i in range(count - 1)])
    high = lax.ppermute(first, "sp", [(i + 1, i) for i in range(count - 1)])
    message = jax.ShapeDtypeStruct((groups, STATE + EXTRA, wide), BF16)
    xc, bc, cc, rows, cols, *sends = pl.pallas_call(
        functools.partial(prepare_kernel, axis="sp"),
        out_shape=[
            jax.ShapeDtypeStruct(x.shape, BF16),
            jax.ShapeDtypeStruct(b.shape, BF16),
            jax.ShapeDtypeStruct(c.shape, BF16),
            jax.ShapeDtypeStruct((2, heads, steps), F32),
            jax.ShapeDtypeStruct((steps, STATE), F32),
        ]
        + [message] * (count - 1),
        in_specs=vmem(11),
        out_specs=vmem(5 + count - 1),
        scratch_shapes=[pltpu.VMEM((steps + 2 * PAD, TILE), F32)],
        name="prepare",
    )(x, b, c, low, high, tx, tb, tc, raw, speed, fade)
    arrived = [
        lax.ppermute(send, "sp", [(i, i ^ k) for i in range(count)])
        for k, send in enumerate(sends, 1)
    ]
    y = pl.pallas_call(
        local_kernel,
        out_shape=jax.ShapeDtypeStruct(x.shape, F32),
        in_specs=vmem(5),
        out_specs=vmem(1)[0],
        cost_estimate=pl.CostEstimate(
            flops=2 * steps * steps * (channels + groups * STATE) * 4,
            bytes_accessed=8 * steps * channels,
            transcendentals=heads * steps * steps,
        ),
        name="local",
    )(xc, bc, cc, rows, cols)
    return pl.pallas_call(
        functools.partial(finish_kernel, axis="sp", minor="tp", rows=block_rows),
        out_shape=[jax.ShapeDtypeStruct((steps // CORES, channels), BF16)] * 2,
        in_specs=vmem(5 + count - 1),
        out_specs=vmem(2),
        scratch_shapes=[pltpu.VMEM((2, STATE, wide), BF16)],
        name="finish",
    )(y, cc, cols, switch, gain.reshape(1, -1), *arrived)


def project_kernel(keep_ref, other_ref, own_w_ref, other_w_ref, *out_refs):
    rows = out_refs[0].shape[0]
    width = own_w_ref.shape[1]
    step = 2 * TILE
    for n in range(0, width, step):
        lanes = slice(n, n + step)
        part = jnp.dot(keep_ref[...], own_w_ref[:, lanes], preferred_element_type=F32) + jnp.dot(
            other_ref[...], other_w_ref[:, lanes], preferred_element_type=F32
        )
        for r, out_ref in enumerate(out_refs):
            out_ref[:, lanes] = part[r * rows : (r + 1) * rows].astype(BF16)


def after_kernel(skip_ref, gain_ref, *refs):
    *part_refs, after_ref, normed_ref = refs
    total = skip_ref[...].astype(F32)
    for ref in part_refs:
        total = total + ref[...].astype(F32)
    after = total.astype(BF16)
    after_ref[...] = after
    values = after.astype(F32)
    mean = jnp.sum(values * values, axis=1, keepdims=True) * (1.0 / values.shape[1])
    normed_ref[...] = (values * lax.rsqrt(mean + EPSILON) * gain_ref[...]).astype(BF16)


def route_kernel(picked_ref, affinity_ref, meta_ref, *, room):
    rows = picked_ref.shape[0]
    lane = lax.broadcasted_iota(jnp.int32, (rows, TILE), 1)
    picks = [jnp.broadcast_to(picked_ref[:, k : k + 1], (rows, TILE)) == lane for k in range(TOP)]
    member = jnp.where(picks[0] | picks[1], 1.0, 0.0)
    earlier = lax.broadcasted_iota(jnp.int32, (rows, rows), 0) > lax.broadcasted_iota(
        jnp.int32, (rows, rows), 1
    )
    rank = jnp.dot(
        jnp.where(earlier, 1.0, 0.0).astype(BF16), member.astype(BF16), preferred_element_type=F32
    )
    affinity = affinity_ref[...]
    total = jnp.sum(affinity, axis=1, keepdims=True)
    meta = jnp.zeros((rows, TILE), F32)
    for k in range(TOP):
        slot = picked_ref[:, k : k + 1].astype(F32) * room + jnp.sum(
            jnp.where(picks[k], rank, 0.0), axis=1, keepdims=True
        )
        meta = jnp.where(lane == k, slot, meta)
        meta = jnp.where(lane == TOP + k, affinity[:, k : k + 1] / total, meta)
    meta_ref[...] = meta


def dispatch_kernel(*refs, chips, room, axis, minor):
    meta_refs, x_refs, out_refs = refs[:chips], refs[chips : 2 * chips], refs[2 * chips :]
    rows, width = x_refs[0].shape
    here = lax.axis_index(axis)
    core = chip_and_core(minor)[1]
    meta = jnp.concatenate([ref[...] for ref in meta_refs], axis=0).T
    rank = lax.broadcasted_iota(jnp.int32, (room, chips * rows), 0).astype(F32)
    source = lax.broadcasted_iota(jnp.int32, (room, chips * rows), 1) // rows
    chosen = []
    for o in range(len(out_refs)):
        expert = (here ^ (o // CORES)) * CORES + (core ^ (o % CORES))
        first = (expert * room).astype(F32)
        hit = (meta[0:1] - first == rank) | (meta[1:2] - first == rank)
        chosen += [
            jnp.where(hit & (source == r), 1.0, 0.0).astype(F32) for r in range(chips)
        ]
    chosen = jnp.concatenate(chosen, axis=0).astype(BF16)
    for n in range(0, width, 2 * TILE):
        lanes = slice(n, n + 2 * TILE)
        tokens = jnp.concatenate([ref[:, lanes] for ref in x_refs], axis=0)
        out = jnp.dot(chosen, tokens, preferred_element_type=F32).astype(BF16)
        for o, ref in enumerate(out_refs):
            ref[:, lanes] = out[o * chips * room : (o + 1) * chips * room]


def combine_kernel(*refs, chips, room, axis, minor):
    meta_refs, in_refs, out_refs = refs[:chips], refs[chips:-chips], refs[-chips:]
    rows, width = out_refs[0].shape
    here = lax.axis_index(axis)
    core = chip_and_core(minor)[1]
    lane = lax.broadcasted_iota(jnp.int32, (rows, chips * room), 1)
    weights = []
    for r in range(chips):
        meta = meta_refs[r][...]
        parts = []
        for o in range(len(in_refs)):
            expert = (here ^ (o // CORES)) * CORES + (core ^ (o % CORES))
            slot = (lane - r * room + expert * room).astype(F32)
            inside = (lane >= r * room) & (lane < (r + 1) * room)
            both = jnp.where(meta[:, 0:1] == slot, meta[:, TOP : TOP + 1], 0.0) + jnp.where(
                meta[:, 1:2] == slot, meta[:, TOP + 1 : TOP + 2], 0.0
            )
            parts.append(jnp.where(inside, both, 0.0).astype(BF16))
        weights.append(parts)
    for n in range(0, width, 2 * TILE):
        lanes = slice(n, n + 2 * TILE)
        total = jnp.zeros((chips * rows, 2 * TILE), F32)
        for o, ref in enumerate(in_refs):
            weight = jnp.concatenate([weights[r][o] for r in range(chips)], axis=0)
            total = total + jnp.dot(weight, ref[:, lanes], preferred_element_type=F32)
        for r, ref in enumerate(out_refs):
            ref[:, lanes] = total[r * rows : (r + 1) * rows].astype(BF16)


def expert_kernel(*refs, count, minor):
    x_refs, weight_refs = refs[:count], refs[count : count + 6]
    out_refs = refs[count + 6 : 2 * count + 6]
    x_vmem, gate_vmem, up_vmem, down_vmem, sum_vmem, sems = refs[2 * count + 6 :]
    core = chip_and_core(minor)[1]
    slabs, _, step = gate_vmem.shape
    per_source = slabs // 2
    copies = []
    for t in range(slabs):
        gate, up, down = weight_refs[0:3] if t < per_source else weight_refs[3:6]
        span = pl.ds((t % per_source) * step, step)
        copies.append(
            [
                pltpu.make_async_copy(gate.at[core, :, span], gate_vmem.at[t], sems.at[t, 0]),
                pltpu.make_async_copy(up.at[core, :, span], up_vmem.at[t], sems.at[t, 1]),
                pltpu.make_async_copy(down.at[core, span, :], down_vmem.at[t], sems.at[t, 2]),
            ]
        )
    for group in copies:
        for copy in group:
            copy.start()
    rows = x_refs[0].shape[0]
    for o, ref in enumerate(x_refs):
        x_vmem[o * rows : (o + 1) * rows, :] = ref[...]
    for t in range(slabs):
        copies[t][0].wait()
        copies[t][1].wait()
        gate = jnp.dot(x_vmem[...], gate_vmem[t], preferred_element_type=F32)
        up = jnp.dot(x_vmem[...], up_vmem[t], preferred_element_type=F32)
        hidden = (silu(gate) * up).astype(BF16)
        copies[t][2].wait()
        width = sum_vmem.shape[1]
        for n in range(0, width, 2 * TILE):
            lanes = slice(n, n + 2 * TILE)
            part = jnp.dot(hidden, down_vmem[t, :, lanes], preferred_element_type=F32)
            if t > 0:
                part = sum_vmem[:, lanes] + part
            if t < slabs - 1:
                sum_vmem[:, lanes] = part
            else:
                for o, ref in enumerate(out_refs):
                    ref[:, lanes] = part[o * rows : (o + 1) * rows].astype(BF16)


def run_experts(messages, own, other):
    count = len(messages)
    rows, width = messages[0].shape
    hidden = own[0].shape[2]
    step = 2 * TILE if hidden % (2 * TILE) == 0 else hidden
    slabs = 2 * (hidden // step)
    return pl.pallas_call(
        functools.partial(expert_kernel, count=count, minor="tp"),
        out_shape=[jax.ShapeDtypeStruct((rows, width), BF16)] * count,
        in_specs=vmem(count) + [pl.BlockSpec(memory_space=pl.ANY)] * 6,
        out_specs=vmem(count),
        scratch_shapes=[
            pltpu.VMEM((count * rows, width), BF16),
            pltpu.VMEM((slabs, width, step), BF16),
            pltpu.VMEM((slabs, width, step), BF16),
            pltpu.VMEM((slabs, step, width), BF16),
            pltpu.VMEM((count * rows, width), F32),
            pltpu.SemaphoreType.DMA((slabs, 3)),
        ],
        cost_estimate=pl.CostEstimate(
            flops=6 * count * rows * width * 2 * hidden,
            bytes_accessed=12 * hidden * width,
            transcendentals=count * rows * 2 * hidden,
        ),
        compiler_params=pltpu.CompilerParams(vmem_limit_bytes=48 * 1024 * 1024),
        name="experts",
    )(*messages, *own, *other)


def per_device(
    skip_stream_entry,
    result_switch_mapped,
    channel_feed_mapped,
    write_coefficient_mapped,
    emission_coefficient_mapped,
    channel_feed_taps,
    write_coefficient_taps,
    emission_coefficient_taps,
    raw_increments,
    channel_log_fade_speed,
    extra_log_fade,
    cluster_scaling_factor,
    blend_result_matrix,
    routing_scaling_factor,
    specialist_switch_matrix,
    specialist_widen_matrix,
    specialist_contract_matrix,
    picked_specialists,
    router_affinities,
):
    rows, width = skip_stream_entry.shape
    peers, minor = lax.axis_size("sp"), lax.axis_size("tp")
    chips = minor // CORES
    assert specialist_switch_matrix.shape[0] == CORES
    experts = CORES * peers
    capacity = max(2, 3 * TOP * rows // (2 * experts))
    room = -(-capacity // 8) * 8

    def to_partner(value):
        return lax.ppermute(value, "tp", [(t, t ^ 1) for t in range(minor)])

    def to_chip(value, ahead):
        return lax.ppermute(
            value, "tp", [(t, (t + CORES * ahead) % minor) for t in range(minor)]
        )

    def to_peer(value, peer, core):
        pairs = [
            (s * minor + t, (s ^ peer) * minor + (t ^ core))
            for s in range(peers)
            for t in range(minor)
        ]
        return lax.ppermute(value, ("sp", "tp"), pairs)

    keep, send = mixer(
        channel_feed_mapped,
        write_coefficient_mapped,
        emission_coefficient_mapped,
        channel_feed_taps,
        write_coefficient_taps,
        emission_coefficient_taps,
        raw_increments,
        channel_log_fade_speed,
        extra_log_fade,
        result_switch_mapped,
        cluster_scaling_factor,
        rows,
    )
    own = (specialist_switch_matrix, specialist_widen_matrix, specialist_contract_matrix)
    other = tuple(to_partner(value) for value in own)
    other_blend = to_partner(blend_result_matrix)
    meta = pl.pallas_call(
        functools.partial(route_kernel, room=room),
        out_shape=jax.ShapeDtypeStruct((rows, TILE), F32),
        in_specs=vmem(2),
        out_specs=vmem(1)[0],
        name="route",
    )(picked_specialists, router_affinities)
    metas = [meta] + [to_chip(meta, r) for r in range(1, chips)]

    piece = jax.ShapeDtypeStruct((rows, width), BF16)
    parts = pl.pallas_call(
        project_kernel,
        out_shape=[piece] * chips,
        in_specs=vmem(4),
        out_specs=vmem(chips),
        name="project",
    )(keep, to_partner(send), blend_result_matrix, other_blend)
    parts = [parts[0]] + [to_chip(parts[r], r) for r in range(1, chips)]
    after, normed = pl.pallas_call(
        after_kernel,
        out_shape=[piece] * 2,
        in_specs=vmem(2 + chips),
        out_specs=vmem(2),
        name="after",
    )(skip_stream_entry, routing_scaling_factor.reshape(1, -1), *parts)

    tokens = [normed] + [to_chip(normed, r) for r in range(1, chips)]
    message = jax.ShapeDtypeStruct((chips * room, width), BF16)
    messages = pl.pallas_call(
        functools.partial(dispatch_kernel, chips=chips, room=room, axis="sp", minor="tp"),
        out_shape=[message] * experts,
        in_specs=vmem(2 * chips),
        out_specs=vmem(experts),
        name="dispatch",
    )(*metas, *tokens)
    messages = [messages[0]] + [
        to_peer(messages[o], o // CORES, o % CORES) for o in range(1, experts)
    ]
    results = run_experts(messages, own, other)
    results = [results[0]] + [
        to_peer(results[o], o // CORES, o % CORES) for o in range(1, experts)
    ]
    sums = pl.pallas_call(
        functools.partial(combine_kernel, chips=chips, room=room, axis="sp", minor="tp"),
        out_shape=[piece] * chips,
        in_specs=vmem(chips + experts),
        out_specs=vmem(chips),
        name="combine",
    )(*metas, *results)
    total = after.astype(F32) + sums[0].astype(F32)
    for r in range(1, chips):
        total = total + to_chip(sums[r], chips - r).astype(F32)
    return total.astype(BF16)


def solution(mesh):
    in_specs = (
        P(("sp", "tp"), None),
        P("sp", "tp"),
        P("sp", "tp"),
        P("sp", "tp"),
        P("sp", "tp"),
        P(None, "tp"),
        P(None, "tp"),
        P(None, "tp"),
        P(None, "tp", "sp"),
        P(None, "tp"),
        P(None, "tp", "sp"),
        P("tp"),
        P("tp", None),
        P(),
        P("sp", None, "tp"),
        P("sp", None, "tp"),
        P("sp", "tp", None),
        P(("sp", "tp"), None),
        P(("sp", "tp"), None),
    )
    out_specs = P(("sp", "tp"), None)
    return jax.shard_map(
        per_device, mesh=mesh, in_specs=in_specs, out_specs=out_specs, check_vma=False
    )
```

```python
import functools
import math

import jax
import jax.numpy as jnp
from jax import lax
from jax.experimental import pallas as pl
from jax.experimental.pallas import tpu as pltpu
from jax.sharding import PartitionSpec as P


HEAD_DIM = 64
STATE = 128
TOP = 2
TILE = 128
PAD = 8
EXTRA = 16

EPSILON = 1e-06
LOG2E = math.log2(math.e)
F32, BF16 = jnp.float32, jnp.bfloat16


CORES = 2
CHUNKS = 2


def chip_and_core(axis):
    at = lax.axis_index(axis)
    return at // CORES, at & (CORES - 1)


def silu(v):
    return v / (1.0 + jnp.exp(-v))


def over_heads(columns, first, count):
    rows = columns.shape[0]
    lane = lax.broadcasted_iota(jnp.int32, (rows, 2 * HEAD_DIM), 1)
    pairs = []
    for h in range(0, count, 2):
        a = jnp.broadcast_to(columns[:, first + h : first + h + 1], lane.shape)
        b = jnp.broadcast_to(columns[:, first + h + 1 : first + h + 2], lane.shape)
        pairs.append(jnp.where(lane < HEAD_DIM, a, b))
    return jnp.concatenate(pairs, axis=1)


def route_kernel(picked_ref, affinity_ref, meta_ref, *, room):
    rows = picked_ref.shape[0]
    lane = lax.broadcasted_iota(jnp.int32, (rows, TILE), 1)
    picks = [jnp.broadcast_to(picked_ref[:, k : k + 1], (rows, TILE)) == lane for k in range(TOP)]
    member = jnp.where(picks[0] | picks[1], 1.0, 0.0)
    earlier = lax.broadcasted_iota(jnp.int32, (rows, rows), 0) > lax.broadcasted_iota(
        jnp.int32, (rows, rows), 1
    )
    rank = jnp.dot(
        jnp.where(earlier, 1.0, 0.0).astype(BF16), member.astype(BF16), preferred_element_type=F32
    )
    affinity = affinity_ref[...]
    total = jnp.sum(affinity, axis=1, keepdims=True)
    meta = jnp.zeros((rows, TILE), F32)
    for k in range(TOP):
        slot = picked_ref[:, k : k + 1].astype(F32) * room + jnp.sum(
            jnp.where(picks[k], rank, 0.0), axis=1, keepdims=True
        )
        meta = jnp.where(lane == k, slot, meta)
        meta = jnp.where(lane == TOP + k, affinity[:, k : k + 1] / total, meta)
    meta_ref[...] = meta


def early_kernel(
    raw_ref, speed_ref, fade_ref, rows_ref, cols_ref, totals_ref
):
    heads, steps = raw_ref.shape[1:]
    lane = lax.broadcasted_iota(jnp.int32, (heads, steps), 1)
    eye = lax.broadcasted_iota(jnp.int32, (heads, heads), 0) == lax.broadcasted_iota(
        jnp.int32, (heads, heads), 1
    )
    sums, weights = [], []
    for d in range(2):
        raw = raw_ref[d].astype(F32)
        step = jnp.maximum(raw, 0.0) + jnp.log1p(jnp.exp(-jnp.abs(raw)))
        speed = jnp.sum(
            jnp.where(eye, jnp.exp(speed_ref[d : d + 1, :]), 0.0), axis=1, keepdims=True
        )
        run = -step * speed + fade_ref[d]
        shift = 1
        while shift < steps:
            if d == 0:
                run = run + jnp.where(lane >= shift, pltpu.roll(run, shift, 1), 0.0)
            else:
                run = run + jnp.where(lane < steps - shift, pltpu.roll(run, steps - shift, 1), 0.0)
            shift *= 2
        total = run[:, steps - 1 : steps] if d == 0 else run[:, 0:1]
        totals_ref[d] = jnp.broadcast_to(total, (heads, STATE))
        sums.append(run * LOG2E)
        weights.append(jnp.exp(total - run) * step)
        rows_ref[d] = run * LOG2E - jnp.log(step) * LOG2E
    stacked = jnp.concatenate(
        sums + weights + [jnp.zeros((STATE - 4 * heads, steps), F32)], axis=0
    )
    cols_ref[...] = stacked.T


def prepare_kernel(
    x_ref, b_ref, c_ref, low_ref, high_ref, tx_ref, tb_ref, tc_ref, cols_ref, totals_ref,
    xc_ref, bc_ref, cc_ref, *rest, axis,
):
    *msg_refs, pad_ref = rest
    steps = x_ref.shape[0]
    heads = totals_ref.shape[1]
    groups = b_ref.shape[1] // STATE
    per_group = heads // groups
    wide = per_group * HEAD_DIM
    here = lax.axis_index(axis)
    cols = cols_ref[...]
    totals = [totals_ref[d, :, 0:1] for d in range(2)]

    def conv(ref, taps_ref, at, start):
        pad_ref[PAD - 2 : PAD] = low_ref[:, at + start : at + start + TILE].astype(F32)
        pad_ref[PAD : PAD + steps] = ref[:, start : start + TILE].astype(F32)
        pad_ref[PAD + steps : PAD + steps + 2] = high_ref[
            :, at + start : at + start + TILE
        ].astype(F32)
        taps = taps_ref[:, start : start + TILE].astype(F32)
        total = taps[0:1] * pad_ref[PAD - 2 : PAD - 2 + steps]
        for j in range(1, taps.shape[0]):
            total = total + taps[j : j + 1] * pad_ref[PAD - 2 + j : PAD - 2 + j + steps]
        return silu(total)

    at = 0
    for ref, taps_ref, out_ref in (
        (x_ref, tx_ref, xc_ref), (b_ref, tb_ref, bc_ref), (c_ref, tc_ref, cc_ref),
    ):
        for start in range(0, ref.shape[1], TILE):
            out_ref[:, start : start + TILE] = conv(ref, taps_ref, at, start).astype(BF16)
        at += ref.shape[1]

    row = lax.broadcasted_iota(jnp.int32, (EXTRA, wide), 0)
    own = lax.broadcasted_iota(jnp.int32, (per_group, wide), 0) == (
        lax.broadcasted_iota(jnp.int32, (per_group, wide), 1) // HEAD_DIM
    )
    for g in range(groups):
        turned = bc_ref[:, g * STATE : (g + 1) * STATE].astype(F32).T.astype(BF16)
        xg = xc_ref[:, g * wide : (g + 1) * wide].astype(F32)
        both = []
        for d in range(2):
            weight = over_heads(cols, (2 + d) * heads + g * per_group, per_group)
            state = jnp.dot(turned, (xg * weight).astype(BF16), preferred_element_type=F32)
            total = jnp.sum(
                jnp.where(own, totals[d][g * per_group : (g + 1) * per_group], 0.0),
                axis=0, keepdims=True,
            )
            upper = total.astype(BF16).astype(F32)
            extra = jnp.where(row == 0, upper, jnp.where(row == 1, total - upper, 0.0))
            both.append((state, extra))
        for k, msg_ref in enumerate(msg_refs, 1):
            onward = jnp.where((here ^ k) > here, 1.0, 0.0).astype(F32)
            (sf, ef), (sb, eb) = both
            msg_ref[g, 0:STATE, :] = (sf * onward + sb * (1.0 - onward)).astype(BF16)
            msg_ref[g, STATE : STATE + EXTRA, :] = (ef * onward + eb * (1.0 - onward)).astype(BF16)


def local_kernel(xc_ref, bc_ref, cc_ref, rows_ref, cols_ref, y_ref):
    steps = xc_ref.shape[0]
    heads = rows_ref.shape[1]
    groups = bc_ref.shape[1] // STATE
    per_group = heads // groups
    tiles = steps // TILE
    i_at = lax.broadcasted_iota(jnp.int32, (TILE, TILE), 0)
    j_at = lax.broadcasted_iota(jnp.int32, (TILE, TILE), 1)
    for g in range(groups):
        for i in range(tiles):
            span = slice(i * TILE, (i + 1) * TILE)
            inner = lax.dot_general(
                cc_ref[span, g * STATE : (g + 1) * STATE],
                bc_ref[:, g * STATE : (g + 1) * STATE],
                (((1,), (1,)), ((), ())),
                preferred_element_type=F32,
            )
            for pair in range(per_group // 2):
                halves = []
                at = (g * per_group + 2 * pair) * HEAD_DIM
                for h in (g * per_group + 2 * pair, g * per_group + 2 * pair + 1):
                    here_f = jnp.broadcast_to(cols_ref[span, h : h + 1], (TILE, TILE))
                    here_b = jnp.broadcast_to(cols_ref[span, heads + h : heads + h + 1], (TILE, TILE))
                    parts = []
                    for j in range(tiles):
                        js = slice(j * TILE, (j + 1) * TILE)
                        if j <= i:
                            mix = jnp.exp2(here_f - rows_ref[0, h : h + 1, js])
                            if j == i:
                                mix = jnp.where(i_at >= j_at, mix, 0.0) + jnp.where(
                                    i_at <= j_at, jnp.exp2(here_b - rows_ref[1, h : h + 1, js]), 0.0
                                )
                        else:
                            mix = jnp.exp2(here_b - rows_ref[1, h : h + 1, js])
                        parts.append((mix * inner[:, js]).astype(BF16))
                    halves.append(
                        jnp.dot(
                            jnp.concatenate(parts, axis=1),
                            xc_ref[:, at : at + 2 * HEAD_DIM],
                            preferred_element_type=F32,
                        )
                    )
                y_ref[span, at : at + 2 * HEAD_DIM] = jnp.where(j_at < HEAD_DIM, *halves)


def finish_kernel(y_ref, cc_ref, cols_ref, switch_ref, gain_ref, *rest, axis, minor, rows):
    *msg_refs, keep_ref, send_ref, carry_ref = rest
    steps, channels = y_ref.shape
    groups = cc_ref.shape[1] // STATE
    wide = channels // groups
    per_group = wide // HEAD_DIM
    heads = groups * per_group
    here = lax.axis_index(axis)
    chip, core = chip_and_core(minor)
    chips = lax.axis_size(minor) // CORES
    peers = [here ^ k for k in range(1, len(msg_refs) + 1)]

    def flag(condition):
        return jnp.where(condition, 1.0, 0.0).astype(F32)

    for g in range(groups):
        totals = [
            ref[g, STATE : STATE + 1, :].astype(F32) + ref[g, STATE + 1 : STATE + 2, :].astype(F32)
            for ref in msg_refs
        ]
        for d in range(2):
            carry = jnp.zeros((STATE, wide), F32)
            for k, ref in enumerate(msg_refs):
                between = jnp.zeros((1, wide), F32)
                for other in range(len(msg_refs)):
                    if other != k:
                        if d == 0:
                            inside = (peers[k] < peers[other]) & (peers[other] < here)
                        else:
                            inside = (peers[k] > peers[other]) & (peers[other] > here)
                        between = between + flag(inside) * totals[other]
                mine = flag(peers[k] < here if d == 0 else peers[k] > here)
                carry = carry + ref[g, 0:STATE, :].astype(F32) * (mine * jnp.exp(between))
            carry_ref[d] = carry.astype(BF16)
        for i in range(steps // TILE):
            span = slice(i * TILE, (i + 1) * TILE)
            lanes = slice(g * wide, (g + 1) * wide)
            cols = jnp.exp2(cols_ref[span, :])
            cc = cc_ref[span, g * STATE : (g + 1) * STATE]
            y = y_ref[span, lanes]
            for d in range(2):
                y = y + over_heads(cols, d * heads + g * per_group, per_group) * jnp.dot(
                    cc, carry_ref[d], preferred_element_type=F32
                )
            gated = y * silu(switch_ref[span, lanes].astype(F32))
            mean = jnp.sum(gated * gated, axis=1, keepdims=True) * (1.0 / wide)
            mixed = gated * lax.rsqrt(mean + EPSILON) * gain_ref[:, lanes]
            for part in range(TILE // (CORES * rows)):
                block = i * (TILE // (CORES * rows)) + part
                south = mixed[part * CORES * rows : (part * CORES + 1) * rows]
                north = mixed[(part * CORES + 1) * rows : (part + 1) * CORES * rows]
                odd = flag(core == 1)
                at = pl.multiple_of(((block - chip) & (chips - 1)) * rows, rows)
                keep_ref[pl.ds(at, rows), lanes] = (south * (1.0 - odd) + north * odd).astype(BF16)
                send_ref[pl.ds(at, rows), lanes] = (south * odd + north * (1.0 - odd)).astype(BF16)


def kernel(body, operands, outs, grant=12, **settings):
    return pl.pallas_call(
        body,
        out_shape=outs,
        out_specs=vmem(len(outs)) if isinstance(outs, list) else vmem(1)[0],
        compiler_params=pltpu.CompilerParams(vmem_limit_bytes=grant * 1024 * 1024),
        **{"in_specs": vmem(len(operands)), **settings},
    )(*operands)


def vmem(count):
    return [pl.BlockSpec(memory_space=pltpu.VMEM) for _ in range(count)]


def mixer(x, b, c, tx, tb, tc, early, switch, gain, block_rows):
    steps, channels = x.shape
    groups = b.shape[1] // STATE
    wide = channels // groups
    rim = tx.shape[0] // 2
    count = lax.axis_size("sp")
    first = jnp.concatenate([x[:rim], b[:rim], c[:rim]], axis=1)
    last = jnp.concatenate([x[-rim:], b[-rim:], c[-rim:]], axis=1)
    low = lax.ppermute(last, "sp", [(i, i + 1) for i in range(count - 1)])
    high = lax.ppermute(first, "sp", [(i + 1, i) for i in range(count - 1)])
    rows, cols, totals = early()
    heads = rows.shape[1]
    message = jax.ShapeDtypeStruct((groups, STATE + EXTRA, wide), BF16)
    xc, bc, cc, *sends = kernel(
        functools.partial(prepare_kernel, axis="sp"),
        (x, b, c, low, high, tx, tb, tc, cols, totals),
        [jax.ShapeDtypeStruct(v.shape, BF16) for v in (x, b, c)] + [message] * (count - 1),
        scratch_shapes=[pltpu.VMEM((steps + 2 * PAD, TILE), F32)],
    )
    arrived = [
        lax.ppermute(send, "sp", [(i, i ^ k) for i in range(count)])
        for k, send in enumerate(sends, 1)
    ]
    y = kernel(
        local_kernel,
        (xc, bc, cc, rows, cols),
        jax.ShapeDtypeStruct(x.shape, F32),
        cost_estimate=pl.CostEstimate(
            flops=2 * steps * steps * (channels + groups * STATE) * 4,
            bytes_accessed=8 * steps * channels,
            transcendentals=heads * steps * steps,
        ),
    )
    return kernel(
        functools.partial(finish_kernel, axis="sp", minor="tp", rows=block_rows),
        (y, cc, cols, switch, gain.reshape(1, -1), *arrived),
        [jax.ShapeDtypeStruct((steps // CORES, channels), BF16)] * 2,
        scratch_shapes=[pltpu.VMEM((2, STATE, wide), BF16)],
    )


def project_kernel(keep_ref, other_ref, own_w_ref, other_w_ref, *out_refs):
    rows = out_refs[0].shape[0]
    width = own_w_ref.shape[1]
    step = 2 * TILE
    for n in range(0, width, step):
        lanes = slice(n, n + step)
        part = jnp.dot(keep_ref[...], own_w_ref[:, lanes], preferred_element_type=F32) + jnp.dot(
            other_ref[...], other_w_ref[:, lanes], preferred_element_type=F32
        )
        for r, out_ref in enumerate(out_refs):
            out_ref[:, lanes] = part[r * rows : (r + 1) * rows].astype(BF16)


def after_kernel(skip_ref, gain_ref, *refs, chips):
    part_refs, (after_ref, *normed_refs) = refs[:chips], refs[chips:]
    total = skip_ref[...].astype(F32)
    for ref in part_refs:
        total = total + ref[...].astype(F32)
    after = total.astype(BF16)
    after_ref[...] = after
    values = after.astype(F32)
    mean = jnp.sum(values * values, axis=1, keepdims=True) * (1.0 / values.shape[1])
    normed = (values * lax.rsqrt(mean + EPSILON) * gain_ref[...]).astype(BF16)
    step = normed_refs[0].shape[1]
    for n, ref in enumerate(normed_refs):
        ref[...] = normed[:, n * step : (n + 1) * step]


def final_kernel(after_ref, *refs, chunks):
    *in_refs, out_ref = refs
    each = len(in_refs) // chunks
    for n in range(chunks):
        step = in_refs[0].shape[1]
        lanes = slice(n * step, (n + 1) * step)
        total = after_ref[:, lanes].astype(F32)
        for ref in in_refs[n * each : (n + 1) * each]:
            total = total + ref[...].astype(F32)
        out_ref[:, lanes] = total.astype(BF16)


def dispatch_kernel(*refs, chips, room, axis, minor):
    meta_refs, x_refs, out_refs = refs[:chips], refs[chips : 2 * chips], refs[2 * chips :]
    rows, width = x_refs[0].shape
    here = lax.axis_index(axis)
    core = chip_and_core(minor)[1]
    meta = jnp.concatenate([ref[...] for ref in meta_refs], axis=0).T
    rank = lax.broadcasted_iota(jnp.int32, (room, chips * rows), 0).astype(F32)
    source = lax.broadcasted_iota(jnp.int32, (room, chips * rows), 1) // rows
    chosen = []
    for o in range(len(out_refs)):
        expert = (here ^ (o // CORES)) * CORES + (core ^ (o % CORES))
        first = (expert * room).astype(F32)
        hit = (meta[0:1] - first == rank) | (meta[1:2] - first == rank)
        chosen += [
            jnp.where(hit & (source == r), 1.0, 0.0).astype(F32) for r in range(chips)
        ]
    chosen = jnp.concatenate(chosen, axis=0).astype(BF16)
    for n in range(0, width, 2 * TILE):
        lanes = slice(n, n + 2 * TILE)
        tokens = jnp.concatenate([ref[:, lanes] for ref in x_refs], axis=0)
        out = jnp.dot(chosen, tokens, preferred_element_type=F32).astype(BF16)
        for o, ref in enumerate(out_refs):
            ref[:, lanes] = out[o * chips * room : (o + 1) * chips * room]


def combine_kernel(*refs, chips, room, axis, minor):
    meta_refs, in_refs, out_refs = refs[:chips], refs[chips:-chips], refs[-chips:]
    rows, width = out_refs[0].shape
    here = lax.axis_index(axis)
    core = chip_and_core(minor)[1]
    lane = lax.broadcasted_iota(jnp.int32, (rows, chips * room), 1)
    weights = []
    for r in range(chips):
        meta = meta_refs[r][...]
        parts = []
        for o in range(len(in_refs)):
            expert = (here ^ (o // CORES)) * CORES + (core ^ (o % CORES))
            slot = (lane - r * room + expert * room).astype(F32)
            inside = (lane >= r * room) & (lane < (r + 1) * room)
            both = jnp.where(meta[:, 0:1] == slot, meta[:, TOP : TOP + 1], 0.0) + jnp.where(
                meta[:, 1:2] == slot, meta[:, TOP + 1 : TOP + 2], 0.0
            )
            parts.append(jnp.where(inside, both, 0.0).astype(BF16))
        weights.append(parts)
    for n in range(0, width, 2 * TILE):
        lanes = slice(n, n + 2 * TILE)
        total = jnp.zeros((chips * rows, 2 * TILE), F32)
        for o, ref in enumerate(in_refs):
            weight = jnp.concatenate([weights[r][o] for r in range(chips)], axis=0)
            total = total + jnp.dot(weight, ref[:, lanes], preferred_element_type=F32)
        for r, ref in enumerate(out_refs):
            ref[:, lanes] = total[r * rows : (r + 1) * rows].astype(BF16)


def hidden_kernel(*refs, count, chunks, minor):
    x_refs, weight_refs, refs = refs[:count], refs[count : count + 4], refs[count + 4 :]
    hidden_ref, x_vmem, gate_vmem, up_vmem, sems = refs
    core = chip_and_core(minor)[1]
    slabs, _, step = gate_vmem.shape
    per_source = slabs // 2
    copies = []
    for t in range(slabs):
        gate, up = weight_refs[0:2] if t < per_source else weight_refs[2:4]
        span = pl.ds((t % per_source) * step, step)
        copies.append(
            [
                pltpu.make_async_copy(gate.at[core, :, span], gate_vmem.at[t], sems.at[t, 0]),
                pltpu.make_async_copy(up.at[core, :, span], up_vmem.at[t], sems.at[t, 1]),
            ]
        )
    for group in copies:
        for copy in group:
            copy.start()
    rows, columns = x_refs[0].shape
    for o, ref in enumerate(x_refs):
        at, n = o // chunks * rows, o % chunks * columns
        x_vmem[at : at + rows, n : n + columns] = ref[...]
    for t in range(slabs):
        for copy in copies[t]:
            copy.wait()
        gate = jnp.dot(x_vmem[...], gate_vmem[t], preferred_element_type=F32)
        up = jnp.dot(x_vmem[...], up_vmem[t], preferred_element_type=F32)
        hidden_ref[:, t * step : (t + 1) * step] = (silu(gate) * up).astype(BF16)


def down_kernel(hidden_ref, own_ref, other_ref, *refs, chunk, minor):
    *out_refs, down_vmem, sems = refs
    core = chip_and_core(minor)[1]
    rows, columns = out_refs[0].shape
    half, step = down_vmem.shape[0] // 2, 2 * TILE
    copies = []
    for n in range(0, columns, step):
        for side, ref in enumerate((own_ref, other_ref)):
            copies.append(
                pltpu.make_async_copy(
                    ref.at[core, :, pl.ds(chunk * columns + n, step)],
                    down_vmem.at[pl.ds(side * half, half), pl.ds(n, step)],
                    sems.at[n // step, side],
                )
            )
    for copy in copies:
        copy.start()
    for n in range(0, columns, step):
        copies[n // step * 2].wait()
        copies[n // step * 2 + 1].wait()
        part = jnp.dot(
            hidden_ref[...], down_vmem[:, n : n + step], preferred_element_type=F32
        ).astype(BF16)
        for o, ref in enumerate(out_refs):
            ref[:, n : n + step] = part[o * rows : (o + 1) * rows]


def run_experts(messages, own, other, chunks):
    flat = [part for message in messages for part in message]
    rows, columns = flat[0].shape
    total_rows, width = len(messages) * rows, columns * chunks
    hidden = own[0].shape[2]
    step = 2 * TILE if hidden % (2 * TILE) == 0 else hidden
    slabs = 2 * (hidden // step)
    inner = kernel(
        functools.partial(hidden_kernel, count=len(flat), chunks=chunks, minor="tp"),
        (*flat, own[0], own[1], other[0], other[1]),
        jax.ShapeDtypeStruct((total_rows, 2 * hidden), BF16),
        grant=28,
        in_specs=vmem(len(flat)) + [pl.BlockSpec(memory_space=pltpu.HBM)] * 4,
        scratch_shapes=[
            pltpu.VMEM((total_rows, width), BF16),
            pltpu.VMEM((slabs, width, step), BF16),
            pltpu.VMEM((slabs, width, step), BF16),
            pltpu.SemaphoreType.DMA((slabs, 2)),
        ],
        cost_estimate=pl.CostEstimate(
            flops=8 * total_rows * width * hidden,
            bytes_accessed=8 * hidden * width,
            transcendentals=total_rows * 2 * hidden,
        ),
    )
    return [
        kernel(
            functools.partial(down_kernel, chunk=n, minor="tp"),
            (inner, own[2], other[2]),
            [jax.ShapeDtypeStruct((rows, columns), BF16)] * len(messages),
            in_specs=vmem(1) + [pl.BlockSpec(memory_space=pltpu.HBM)] * 2,
            scratch_shapes=[
                pltpu.VMEM((2 * hidden, columns), BF16),
                pltpu.SemaphoreType.DMA((columns // (2 * TILE), 2)),
            ],
            cost_estimate=pl.CostEstimate(
                flops=4 * total_rows * columns * hidden,
                bytes_accessed=4 * hidden * columns,
                transcendentals=0,
            ),
        )
        for n in range(chunks)
    ]


def per_device(
    skip_stream_entry,
    result_switch_mapped,
    channel_feed_mapped,
    write_coefficient_mapped,
    emission_coefficient_mapped,
    channel_feed_taps,
    write_coefficient_taps,
    emission_coefficient_taps,
    raw_increments,
    channel_log_fade_speed,
    extra_log_fade,
    cluster_scaling_factor,
    blend_result_matrix,
    routing_scaling_factor,
    specialist_switch_matrix,
    specialist_widen_matrix,
    specialist_contract_matrix,
    picked_specialists,
    router_affinities,
):
    rows, width = skip_stream_entry.shape
    peers, minor = lax.axis_size("sp"), lax.axis_size("tp")
    chips = minor // CORES
    assert specialist_switch_matrix.shape[0] == CORES
    experts = CORES * peers
    capacity = max(2, 3 * TOP * rows // (2 * experts))
    room = -(-capacity // 8) * 8

    def to_partner(value):
        return lax.ppermute(value, "tp", [(t, t ^ 1) for t in range(minor)])

    def to_chip(value, ahead):
        pairs = [(t, (t + CORES * ahead) % minor) for t in range(minor)]
        return lax.ppermute(value, "tp", pairs)

    def to_peer(value, o):
        pairs = [
            (s * minor + t, (s ^ (o // CORES)) * minor + (t ^ (o % CORES)))
            for s in range(peers)
            for t in range(minor)
        ]
        return lax.ppermute(value, ("sp", "tp"), pairs)

    piece = jax.ShapeDtypeStruct((rows, width), BF16)
    slim = jax.ShapeDtypeStruct((rows, width // CHUNKS), BF16)
    message = jax.ShapeDtypeStruct((chips * room, width // CHUNKS), BF16)

    def early():
        return kernel(
            early_kernel,
            (raw_increments, channel_log_fade_speed, extra_log_fade),
            [
                jax.ShapeDtypeStruct(raw_increments.shape, F32),
                jax.ShapeDtypeStruct((raw_increments.shape[2], STATE), F32),
                jax.ShapeDtypeStruct((*raw_increments.shape[:2], STATE), F32),
            ],
        )

    keep, send = mixer(
        channel_feed_mapped,
        write_coefficient_mapped,
        emission_coefficient_mapped,
        channel_feed_taps,
        write_coefficient_taps,
        emission_coefficient_taps,
        early,
        result_switch_mapped,
        cluster_scaling_factor,
        rows,
    )
    own = (specialist_switch_matrix, specialist_widen_matrix, specialist_contract_matrix)
    other = tuple(to_partner(value) for value in own)
    parts = kernel(
        project_kernel,
        (keep, to_partner(send), blend_result_matrix, to_partner(blend_result_matrix)),
        [piece] * chips,
    )
    parts = [parts[0]] + [to_chip(parts[r], r) for r in range(1, chips)]
    after, *normed = kernel(
        functools.partial(after_kernel, chips=chips),
        (skip_stream_entry, routing_scaling_factor.reshape(1, -1), *parts),
        [piece] + [slim] * CHUNKS,
    )
    meta = kernel(
        functools.partial(route_kernel, room=room),
        (picked_specialists, router_affinities),
        jax.ShapeDtypeStruct((rows, TILE), F32),
    )
    metas = [meta] + [to_chip(meta, r) for r in range(1, chips)]
    places = dict(chips=chips, room=room, axis="sp", minor="tp")
    messages = []
    for n in range(CHUNKS):
        tokens = [normed[n]] + [to_chip(normed[n], r) for r in range(1, chips)]
        sends = kernel(
            functools.partial(dispatch_kernel, **places), (*metas, *tokens), [message] * experts
        )
        messages.append([sends[0]] + [to_peer(sends[o], o) for o in range(1, experts)])
    bounds = group_bounds(peers)
    results = [[] for _ in range(CHUNKS)]
    for first, last in zip(bounds[:-1], bounds[1:]):
        part = [[messages[n][o] for n in range(CHUNKS)] for o in range(first, last)]
        done = run_experts(part, own, other, CHUNKS)
        for n in range(CHUNKS):
            results[n] += done[n]
    pieces = []
    for n in range(CHUNKS):
        back = [results[n][0]] + [to_peer(results[n][o], o) for o in range(1, experts)]
        sums = kernel(functools.partial(combine_kernel, **places), (*metas, *back), [slim] * chips)
        pieces += [sums[0]] + [to_chip(sums[chips - r], r) for r in range(1, chips)]
    return kernel(functools.partial(final_kernel, chunks=CHUNKS), (after, *pieces), piece)


def group_bounds(peers):
    return [0, CORES, CORES * peers]


def solution(mesh):
    in_specs = (
        P(("sp", "tp"), None),
        P("sp", "tp"),
        P("sp", "tp"),
        P("sp", "tp"),
        P("sp", "tp"),
        P(None, "tp"),
        P(None, "tp"),
        P(None, "tp"),
        P(None, "tp", "sp"),
        P(None, "tp"),
        P(None, "tp", "sp"),
        P("tp"),
        P("tp", None),
        P(),
        P("sp", None, "tp"),
        P("sp", None, "tp"),
        P("sp", "tp", None),
        P(("sp", "tp"), None),
        P(("sp", "tp"), None),
    )
    out_specs = P(("sp", "tp"), None)

    return jax.shard_map(
        per_device, mesh=mesh, in_specs=in_specs, out_specs=out_specs, check_vma=False
    )
```

```python
import functools
import math

import jax
import jax.numpy as jnp
from jax import lax
from jax.experimental import pallas as pl
from jax.experimental.pallas import tpu as pltpu
from jax.sharding import PartitionSpec as P


HEAD_DIM = 64
STATE = 128
TOP = 2
TILE = 128
PAD = 8
SPREAD = 2
EXTRA = 16

EPSILON = 1e-06
LOG2E = math.log2(math.e)
F32, BF16 = jnp.float32, jnp.bfloat16


CORES = 2
CHUNKS = 2


def chunk_widths(width):
    last = max(width // 8 // (2 * TILE), 1) * 2 * TILE * SPREAD
    second = (width - last) // 2 // (2 * TILE) * 2 * TILE
    return (width - last - second, second, last)


def chip_and_core(axis):
    at = lax.axis_index(axis)
    return at // CORES, at & (CORES - 1)


def silu(v):
    return v / (1.0 + jnp.exp(-v))


def over_heads(columns, first, count):
    rows = columns.shape[0]
    lane = lax.broadcasted_iota(jnp.int32, (rows, 2 * HEAD_DIM), 1)
    pairs = []
    for h in range(0, count, 2):
        a = jnp.broadcast_to(columns[:, first + h : first + h + 1], lane.shape)
        b = jnp.broadcast_to(columns[:, first + h + 1 : first + h + 2], lane.shape)
        pairs.append(jnp.where(lane < HEAD_DIM, a, b))
    return jnp.concatenate(pairs, axis=1)


def route_kernel(picked_ref, affinity_ref, meta_ref, *, room):
    rows = picked_ref.shape[0]
    lane = lax.broadcasted_iota(jnp.int32, (rows, TILE), 1)
    picks = [jnp.broadcast_to(picked_ref[:, k : k + 1], (rows, TILE)) == lane for k in range(TOP)]
    member = jnp.where(picks[0] | picks[1], 1.0, 0.0)
    earlier = lax.broadcasted_iota(jnp.int32, (rows, rows), 0) > lax.broadcasted_iota(
        jnp.int32, (rows, rows), 1
    )
    rank = jnp.dot(
        jnp.where(earlier, 1.0, 0.0).astype(BF16), member.astype(BF16), preferred_element_type=F32
    )
    affinity = affinity_ref[...]
    total = jnp.sum(affinity, axis=1, keepdims=True)
    meta = jnp.zeros((rows, TILE), F32)
    for k in range(TOP):
        slot = picked_ref[:, k : k + 1].astype(F32) * room + jnp.sum(
            jnp.where(picks[k], rank, 0.0), axis=1, keepdims=True
        )
        meta = jnp.where(lane == k, slot, meta)
        meta = jnp.where(lane == TOP + k, affinity[:, k : k + 1] / total, meta)
    meta_ref[...] = meta


def early_kernel(
    raw_hbm, speed_hbm, fade_hbm, *refs,
):
    count = (len(refs) - 7) // 2
    in_refs, out_refs = refs[:count], refs[count : 2 * count]
    rows_ref, cols_ref, totals_ref, raw_ref, speed_ref, fade_ref, sems = refs[2 * count :]
    pairs = [(raw_hbm, raw_ref), (speed_hbm, speed_ref), (fade_hbm, fade_ref)]
    pairs += list(zip(in_refs, out_refs))
    copies = [pltpu.make_async_copy(a, b, sems.at[n]) for n, (a, b) in enumerate(pairs)]
    for copy in copies:
        copy.start()
    for copy in copies[:3]:
        copy.wait()
    heads, steps = raw_ref.shape[1:]
    lane = lax.broadcasted_iota(jnp.int32, (heads, steps), 1)
    eye = lax.broadcasted_iota(jnp.int32, (heads, heads), 0) == lax.broadcasted_iota(
        jnp.int32, (heads, heads), 1
    )
    sums, weights = [], []
    for d in range(2):
        raw = raw_ref[d].astype(F32)
        step = jnp.maximum(raw, 0.0) + jnp.log1p(jnp.exp(-jnp.abs(raw)))
        speed = jnp.sum(
            jnp.where(eye, jnp.exp(speed_ref[d : d + 1, :]), 0.0), axis=1, keepdims=True
        )
        run = -step * speed + fade_ref[d]
        shift = 1
        while shift < steps:
            if d == 0:
                run = run + jnp.where(lane >= shift, pltpu.roll(run, shift, 1), 0.0)
            else:
                run = run + jnp.where(lane < steps - shift, pltpu.roll(run, steps - shift, 1), 0.0)
            shift *= 2
        total = run[:, steps - 1 : steps] if d == 0 else run[:, 0:1]
        totals_ref[d] = jnp.broadcast_to(total, (heads, STATE))
        sums.append(run * LOG2E)
        weights.append(jnp.exp(total - run) * step)
        rows_ref[d] = run * LOG2E - jnp.log(step) * LOG2E
    stacked = jnp.concatenate(
        sums + weights + [jnp.zeros((STATE - 4 * heads, steps), F32)], axis=0
    )
    cols_ref[...] = stacked.T
    for copy in copies[3:]:
        copy.wait()


def prepare_kernel(
    x_ref, b_ref, c_ref, low_ref, high_ref, tx_ref, tb_ref, tc_ref, cols_ref, totals_ref,
    xc_ref, bc_ref, cc_ref, *rest, axis,
):
    *msg_refs, pad_ref = rest
    steps = x_ref.shape[0]
    heads = totals_ref.shape[1]
    groups = b_ref.shape[1] // STATE
    per_group = heads // groups
    wide = per_group * HEAD_DIM
    here = lax.axis_index(axis)
    cols = cols_ref[...]
    totals = [totals_ref[d, :, 0:1] for d in range(2)]

    def conv(ref, taps_ref, at, start):
        pad_ref[PAD - 2 : PAD] = low_ref[:, at + start : at + start + TILE].astype(F32)
        pad_ref[PAD : PAD + steps] = ref[:, start : start + TILE].astype(F32)
        pad_ref[PAD + steps : PAD + steps + 2] = high_ref[
            :, at + start : at + start + TILE
        ].astype(F32)
        taps = taps_ref[:, start : start + TILE].astype(F32)
        total = taps[0:1] * pad_ref[PAD - 2 : PAD - 2 + steps]
        for j in range(1, taps.shape[0]):
            total = total + taps[j : j + 1] * pad_ref[PAD - 2 + j : PAD - 2 + j + steps]
        return silu(total)

    at = 0
    for ref, taps_ref, out_ref in (
        (x_ref, tx_ref, xc_ref), (b_ref, tb_ref, bc_ref), (c_ref, tc_ref, cc_ref),
    ):
        for start in range(0, ref.shape[1], TILE):
            out_ref[:, start : start + TILE] = conv(ref, taps_ref, at, start).astype(BF16)
        at += ref.shape[1]

    row = lax.broadcasted_iota(jnp.int32, (EXTRA, wide), 0)
    own = lax.broadcasted_iota(jnp.int32, (per_group, wide), 0) == (
        lax.broadcasted_iota(jnp.int32, (per_group, wide), 1) // HEAD_DIM
    )
    for g in range(groups):
        turned = bc_ref[:, g * STATE : (g + 1) * STATE].astype(F32).T.astype(BF16)
        xg = xc_ref[:, g * wide : (g + 1) * wide].astype(F32)
        both = []
        for d in range(2):
            weight = over_heads(cols, (2 + d) * heads + g * per_group, per_group)
            state = jnp.dot(turned, (xg * weight).astype(BF16), preferred_element_type=F32)
            total = jnp.sum(
                jnp.where(own, totals[d][g * per_group : (g + 1) * per_group], 0.0),
                axis=0, keepdims=True,
            )
            upper = total.astype(BF16).astype(F32)
            extra = jnp.where(row == 0, upper, jnp.where(row == 1, total - upper, 0.0))
            both.append((state, extra))
        for k, msg_ref in enumerate(msg_refs, 1):
            onward = jnp.where((here ^ k) > here, 1.0, 0.0).astype(F32)
            (sf, ef), (sb, eb) = both
            msg_ref[g, 0:STATE, :] = (sf * onward + sb * (1.0 - onward)).astype(BF16)
            msg_ref[g, STATE : STATE + EXTRA, :] = (ef * onward + eb * (1.0 - onward)).astype(BF16)


def local_kernel(xc_ref, bc_ref, cc_ref, rows_ref, cols_ref, y_ref):
    steps = xc_ref.shape[0]
    heads = rows_ref.shape[1]
    groups = bc_ref.shape[1] // STATE
    per_group = heads // groups
    tiles = steps // TILE
    i_at = lax.broadcasted_iota(jnp.int32, (TILE, TILE), 0)
    j_at = lax.broadcasted_iota(jnp.int32, (TILE, TILE), 1)
    for g in range(groups):
        for i in range(tiles):
            span = slice(i * TILE, (i + 1) * TILE)
            inner = lax.dot_general(
                cc_ref[span, g * STATE : (g + 1) * STATE],
                bc_ref[:, g * STATE : (g + 1) * STATE],
                (((1,), (1,)), ((), ())),
                preferred_element_type=F32,
            )
            for pair in range(per_group // 2):
                halves = []
                at = (g * per_group + 2 * pair) * HEAD_DIM
                for h in (g * per_group + 2 * pair, g * per_group + 2 * pair + 1):
                    here_f = jnp.broadcast_to(cols_ref[span, h : h + 1], (TILE, TILE))
                    here_b = jnp.broadcast_to(cols_ref[span, heads + h : heads + h + 1], (TILE, TILE))
                    parts = []
                    for j in range(tiles):
                        js = slice(j * TILE, (j + 1) * TILE)
                        if j <= i:
                            mix = jnp.exp2(here_f - rows_ref[0, h : h + 1, js])
                            if j == i:
                                mix = jnp.where(i_at >= j_at, mix, 0.0) + jnp.where(
                                    i_at <= j_at, jnp.exp2(here_b - rows_ref[1, h : h + 1, js]), 0.0
                                )
                        else:
                            mix = jnp.exp2(here_b - rows_ref[1, h : h + 1, js])
                        parts.append((mix * inner[:, js]).astype(BF16))
                    halves.append(
                        jnp.dot(
                            jnp.concatenate(parts, axis=1),
                            xc_ref[:, at : at + 2 * HEAD_DIM],
                            preferred_element_type=F32,
                        )
                    )
                y_ref[span, at : at + 2 * HEAD_DIM] = jnp.where(j_at < HEAD_DIM, *halves)


def finish_kernel(y_ref, cc_ref, cols_ref, switch_ref, gain_ref, *rest, axis, minor, rows):
    *msg_refs, keep_ref, send_ref, carry_ref = rest
    steps, channels = y_ref.shape
    groups = cc_ref.shape[1] // STATE
    wide = channels // groups
    per_group = wide // HEAD_DIM
    heads = groups * per_group
    here = lax.axis_index(axis)
    chip, core = chip_and_core(minor)
    chips = lax.axis_size(minor) // CORES
    peers = [here ^ k for k in range(1, len(msg_refs) + 1)]

    def flag(condition):
        return jnp.where(condition, 1.0, 0.0).astype(F32)

    for g in range(groups):
        totals = [
            ref[g, STATE : STATE + 1, :].astype(F32) + ref[g, STATE + 1 : STATE + 2, :].astype(F32)
            for ref in msg_refs
        ]
        for d in range(2):
            carry = jnp.zeros((STATE, wide), F32)
            for k, ref in enumerate(msg_refs):
                between = jnp.zeros((1, wide), F32)
                for other in range(len(msg_refs)):
                    if other != k:
                        if d == 0:
                            inside = (peers[k] < peers[other]) & (peers[other] < here)
                        else:
                            inside = (peers[k] > peers[other]) & (peers[other] > here)
                        between = between + flag(inside) * totals[other]
                mine = flag(peers[k] < here if d == 0 else peers[k] > here)
                carry = carry + ref[g, 0:STATE, :].astype(F32) * (mine * jnp.exp(between))
            carry_ref[d] = carry.astype(BF16)
        for i in range(steps // TILE):
            span = slice(i * TILE, (i + 1) * TILE)
            lanes = slice(g * wide, (g + 1) * wide)
            cols = jnp.exp2(cols_ref[span, :])
            cc = cc_ref[span, g * STATE : (g + 1) * STATE]
            y = y_ref[span, lanes]
            for d in range(2):
                y = y + over_heads(cols, d * heads + g * per_group, per_group) * jnp.dot(
                    cc, carry_ref[d], preferred_element_type=F32
                )
            gated = y * silu(switch_ref[span, lanes].astype(F32))
            mean = jnp.sum(gated * gated, axis=1, keepdims=True) * (1.0 / wide)
            mixed = gated * lax.rsqrt(mean + EPSILON) * gain_ref[:, lanes]
            for part in range(TILE // (CORES * rows)):
                block = i * (TILE // (CORES * rows)) + part
                south = mixed[part * CORES * rows : (part * CORES + 1) * rows]
                north = mixed[(part * CORES + 1) * rows : (part + 1) * CORES * rows]
                odd = flag(core == 1)
                at = pl.multiple_of(((block - chip) & (chips - 1)) * rows, rows)
                keep_ref[pl.ds(at, rows), lanes] = (south * (1.0 - odd) + north * odd).astype(BF16)
                send_ref[pl.ds(at, rows), lanes] = (south * odd + north * (1.0 - odd)).astype(BF16)


def kernel(body, operands, outs, grant=12, **settings):
    return pl.pallas_call(
        body,
        out_shape=outs,
        out_specs=vmem(len(outs)) if isinstance(outs, list) else vmem(1)[0],
        compiler_params=pltpu.CompilerParams(vmem_limit_bytes=grant * 1024 * 1024),
        **({} if "in_specs" in settings else dict(in_specs=vmem(len(operands)))),
        **settings,
    )(*operands)


def vmem(count):
    return [pl.BlockSpec(memory_space=pltpu.VMEM) for _ in range(count)]


def mixer(x, b, c, tx, tb, tc, early, switch, gain, block_rows):
    steps, channels = x.shape
    groups = b.shape[1] // STATE
    wide = channels // groups
    rim = tx.shape[0] // 2
    count = lax.axis_size("sp")
    first = jnp.concatenate([x[:rim], b[:rim], c[:rim]], axis=1)
    last = jnp.concatenate([x[-rim:], b[-rim:], c[-rim:]], axis=1)
    low = lax.ppermute(last, "sp", [(i, i + 1) for i in range(count - 1)])
    high = lax.ppermute(first, "sp", [(i + 1, i) for i in range(count - 1)])
    x, b, c, tx, tb, tc, rows, cols, totals = early(x, b, c, tx, tb, tc)
    heads = rows.shape[1]
    message = jax.ShapeDtypeStruct((groups, STATE + EXTRA, wide), BF16)
    xc, bc, cc, *sends = kernel(
        functools.partial(prepare_kernel, axis="sp"),
        (x, b, c, low, high, tx, tb, tc, cols, totals),
        [jax.ShapeDtypeStruct(v.shape, BF16) for v in (x, b, c)] + [message] * (count - 1),
        scratch_shapes=[pltpu.VMEM((steps + 2 * PAD, TILE), F32)],
    )
    arrived = [
        lax.ppermute(send, "sp", [(i, i ^ k) for i in range(count)])
        for k, send in enumerate(sends, 1)
    ]
    y = kernel(
        local_kernel,
        (xc, bc, cc, rows, cols),
        jax.ShapeDtypeStruct(x.shape, F32),
        cost_estimate=pl.CostEstimate(
            flops=2 * steps * steps * (channels + groups * STATE) * 4,
            bytes_accessed=8 * steps * channels,
            transcendentals=heads * steps * steps,
        ),
    )
    return kernel(
        functools.partial(finish_kernel, axis="sp", minor="tp", rows=block_rows),
        (y, cc, cols, switch, gain.reshape(1, -1), *arrived),
        [jax.ShapeDtypeStruct((steps // CORES, channels), BF16)] * 2,
        scratch_shapes=[pltpu.VMEM((2, STATE, wide), BF16)],
    )


def project_kernel(keep_ref, other_ref, own_w_ref, other_w_ref, *out_refs):
    rows = out_refs[0].shape[0]
    width = own_w_ref.shape[1]
    step = 2 * TILE
    for n in range(0, width, step):
        lanes = slice(n, n + step)
        part = jnp.dot(keep_ref[...], own_w_ref[:, lanes], preferred_element_type=F32) + jnp.dot(
            other_ref[...], other_w_ref[:, lanes], preferred_element_type=F32
        )
        for r, out_ref in enumerate(out_refs):
            out_ref[:, lanes] = part[r * rows : (r + 1) * rows].astype(BF16)


def after_kernel(skip_ref, gain_ref, *refs, chips):
    part_refs, (after_ref, *normed_refs) = refs[:chips], refs[chips:]
    total = skip_ref[...].astype(F32)
    for ref in part_refs:
        total = total + ref[...].astype(F32)
    after = total.astype(BF16)
    after_ref[...] = after
    values = after.astype(F32)
    mean = jnp.sum(values * values, axis=1, keepdims=True) * (1.0 / values.shape[1])
    normed = (values * lax.rsqrt(mean + EPSILON) * gain_ref[...]).astype(BF16)
    at = 0
    for ref in normed_refs:
        ref[...] = normed[:, at : at + ref.shape[1]]
        at += ref.shape[1]


def final_kernel(after_ref, *refs, counts):
    *in_refs, out_ref = refs
    at = 0
    for count in counts:
        part_refs, in_refs = in_refs[:count], in_refs[count:]
        lanes = slice(at, at + part_refs[0].shape[1])
        total = after_ref[:, lanes].astype(F32)
        for ref in part_refs:
            total = total + ref[...].astype(F32)
        out_ref[:, lanes] = total.astype(BF16)
        at = lanes.stop


def regroup_kernel(*refs, count, parts):
    in_refs, out_refs = refs[:count], refs[count:]
    rows = in_refs[0].shape[0] // parts
    values = [ref[...].astype(F32) for ref in in_refs]
    for n, ref in enumerate(out_refs):
        span = slice(n * rows, (n + 1) * rows)
        ref[...] = jnp.concatenate([value[span] for value in values], axis=0).astype(BF16)


def spread_kernel(*refs, count):
    total = refs[0][...].astype(F32)
    for ref in refs[1:count]:
        total = total + ref[...].astype(F32)
    for n, ref in enumerate(refs[count:]):
        rows = ref.shape[0]
        ref[...] = total[n * rows : (n + 1) * rows].astype(BF16)


def own_combine_kernel(meta_ref, *refs, room, axis, minor):
    *in_refs, out_ref = refs
    rows = out_ref.shape[0]
    here = lax.axis_index(axis)
    core = chip_and_core(minor)[1]
    meta = meta_ref[...]
    lane = lax.broadcasted_iota(jnp.int32, (rows, len(in_refs) * room), 1)
    slot = lane
    for o in range(len(in_refs)):
        expert = (here ^ (o // CORES)) * CORES + (core ^ (o % CORES))
        inside = (lane >= o * room) & (lane < (o + 1) * room)
        slot = jnp.where(inside, lane + (expert - o) * room, slot)
    slot = slot.astype(F32)
    weight = jnp.where(meta[:, 0:1] == slot, meta[:, TOP : TOP + 1], 0.0) + jnp.where(
        meta[:, 1:2] == slot, meta[:, TOP + 1 : TOP + 2], 0.0
    )
    values = jnp.concatenate([ref[...].astype(F32) for ref in in_refs], axis=0).astype(BF16)
    out_ref[...] = jnp.dot(
        weight.astype(BF16), values, preferred_element_type=F32
    ).astype(BF16)


def dispatch_kernel(*refs, chips, room, axis, minor):
    meta_refs, x_refs, out_refs = refs[:chips], refs[chips : 2 * chips], refs[2 * chips :]
    rows, width = x_refs[0].shape
    here = lax.axis_index(axis)
    core = chip_and_core(minor)[1]
    lanes_used = max(chips * rows, TILE)
    spare = lanes_used - chips * rows
    metas = [ref[...] for ref in meta_refs]
    if spare:
        metas.append(jnp.zeros((spare, TILE), F32))
    meta = jnp.concatenate(metas, axis=0).T
    rank = lax.broadcasted_iota(jnp.int32, (room, lanes_used), 0).astype(F32)
    source = lax.broadcasted_iota(jnp.int32, (room, lanes_used), 1) // rows
    chosen = []
    for o in range(len(out_refs)):
        expert = (here ^ (o // CORES)) * CORES + (core ^ (o % CORES))
        first = (expert * room).astype(F32)
        hit = (meta[0:1] - first == rank) | (meta[1:2] - first == rank)
        chosen += [
            jnp.where(hit & (source == r), 1.0, 0.0).astype(F32) for r in range(chips)
        ]
    chosen = jnp.concatenate(chosen, axis=0).astype(BF16)
    for n in range(0, width, 2 * TILE):
        lanes = slice(n, n + 2 * TILE)
        tokens = [ref[:, lanes] for ref in x_refs]
        if spare:
            tokens.append(jnp.zeros((spare, 2 * TILE), BF16))
        tokens = jnp.concatenate(tokens, axis=0)
        out = jnp.dot(chosen, tokens, preferred_element_type=F32)
        for o, ref in enumerate(out_refs):
            ref[:, lanes] = out[o * chips * room : (o + 1) * chips * room].astype(BF16)


def combine_kernel(*refs, chips, room, axis, minor):
    meta_refs, in_refs, out_refs = refs[:chips], refs[chips:-chips], refs[-chips:]
    rows, width = out_refs[0].shape
    here = lax.axis_index(axis)
    core = chip_and_core(minor)[1]
    lane = lax.broadcasted_iota(jnp.int32, (rows, chips * room), 1)
    weights = []
    for r in range(chips):
        meta = meta_refs[r][...]
        parts = []
        for o in range(len(in_refs)):
            expert = (here ^ (o // CORES)) * CORES + (core ^ (o % CORES))
            slot = (lane - r * room + expert * room).astype(F32)
            inside = (lane >= r * room) & (lane < (r + 1) * room)
            both = jnp.where(meta[:, 0:1] == slot, meta[:, TOP : TOP + 1], 0.0) + jnp.where(
                meta[:, 1:2] == slot, meta[:, TOP + 1 : TOP + 2], 0.0
            )
            parts.append(jnp.where(inside, both, 0.0).astype(BF16))
        weights.append(parts)
    for n in range(0, width, 2 * TILE):
        lanes = slice(n, n + 2 * TILE)
        total = jnp.zeros((chips * rows, 2 * TILE), F32)
        for o, ref in enumerate(in_refs):
            weight = jnp.concatenate([weights[r][o] for r in range(chips)], axis=0)
            total = total + jnp.dot(weight, ref[:, lanes], preferred_element_type=F32)
        for r, ref in enumerate(out_refs):
            ref[:, lanes] = total[r * rows : (r + 1) * rows].astype(BF16)


def weights_kernel(*refs, minor):
    in_refs, (gate_ref, up_ref, down_ref, sems) = refs[:6], refs[6:]
    core = chip_and_core(minor)[1]
    slabs, _, step = gate_ref.shape
    per_source = slabs // 2
    half = down_ref.shape[0] // 2
    copies = []
    for side in range(2):
        gate, up, down = in_refs[3 * side : 3 * side + 3]
        for t in range(per_source):
            at, span = side * per_source + t, pl.ds(t * step, step)
            copies.append((gate.at[core, :, span], gate_ref.at[at]))
            copies.append((up.at[core, :, span], up_ref.at[at]))
        copies.append((down.at[core], down_ref.at[pl.ds(side * half, half)]))
    copies = [pltpu.make_async_copy(a, b, sems.at[n]) for n, (a, b) in enumerate(copies)]
    for copy in copies:
        copy.start()
    for copy in copies:
        copy.wait()


def hidden_kernel(*refs, count, chunks):
    x_refs, (gate_ref, up_ref, hidden_ref, x_vmem) = refs[:count], refs[count:]
    slabs, _, step = gate_ref.shape
    rows, at = x_refs[0].shape[0], 0
    for n in range(chunks):
        columns = x_refs[n].shape[1]
        for o, ref in enumerate(x_refs[n::chunks]):
            x_vmem[o * rows : (o + 1) * rows, at : at + columns] = ref[...]
        at += columns
    for t in range(slabs):
        gate = jnp.dot(x_vmem[...], gate_ref[t], preferred_element_type=F32)
        up = jnp.dot(x_vmem[...], up_ref[t], preferred_element_type=F32)
        hidden_ref[:, t * step : (t + 1) * step] = (silu(gate) * up).astype(BF16)


def down_kernel(hidden_ref, down_ref, *out_refs, first):
    rows, columns = out_refs[0].shape
    for n in range(0, columns, 2 * TILE):
        at = first + n
        part = jnp.dot(
            hidden_ref[...], down_ref[:, at : at + 2 * TILE], preferred_element_type=F32
        ).astype(BF16)
        for o, ref in enumerate(out_refs):
            ref[:, n : n + 2 * TILE] = part[o * rows : (o + 1) * rows]


def side_by_side(own, other):
    _, width, hidden = own[0].shape
    step = 2 * TILE if hidden % (2 * TILE) == 0 else hidden
    slabs = 2 * (hidden // step)
    return kernel(
        functools.partial(weights_kernel, minor="tp"),
        (*own, *other),
        [jax.ShapeDtypeStruct((slabs, width, step), BF16)] * 2
        + [jax.ShapeDtypeStruct((2 * hidden, width), BF16)],
        grant=28,
        in_specs=[pl.BlockSpec(memory_space=pltpu.HBM)] * 6,
        scratch_shapes=[pltpu.SemaphoreType.DMA((2 * slabs + 2,))],
    )


def run_experts(messages, gate, up, down):
    flat = [part for message in messages for part in message]
    widths = [part.shape[1] for part in messages[0]]
    rows, width = flat[0].shape[0], sum(widths)
    total_rows, hidden = len(messages) * rows, down.shape[0]
    inner = kernel(
        functools.partial(hidden_kernel, count=len(flat), chunks=len(widths)),
        (*flat, gate, up),
        jax.ShapeDtypeStruct((total_rows, hidden), BF16),
        grant=24,
        scratch_shapes=[pltpu.VMEM((total_rows, width), BF16)],
        cost_estimate=pl.CostEstimate(
            flops=4 * total_rows * width * hidden,
            bytes_accessed=4 * hidden * width,
            transcendentals=total_rows * hidden,
        ),
    )
    return [
        kernel(
            functools.partial(down_kernel, first=sum(widths[:n])),
            (inner, down),
            [jax.ShapeDtypeStruct((rows, columns), BF16)] * len(messages),
            cost_estimate=pl.CostEstimate(
                flops=2 * total_rows * columns * hidden,
                bytes_accessed=2 * hidden * columns,
                transcendentals=0,
            ),
        )
        for n, columns in enumerate(widths)
    ]


def per_device(
    skip_stream_entry,
    result_switch_mapped,
    channel_feed_mapped,
    write_coefficient_mapped,
    emission_coefficient_mapped,
    channel_feed_taps,
    write_coefficient_taps,
    emission_coefficient_taps,
    raw_increments,
    channel_log_fade_speed,
    extra_log_fade,
    cluster_scaling_factor,
    blend_result_matrix,
    routing_scaling_factor,
    specialist_switch_matrix,
    specialist_widen_matrix,
    specialist_contract_matrix,
    picked_specialists,
    router_affinities,
):
    rows, width = skip_stream_entry.shape
    peers, minor = lax.axis_size("sp"), lax.axis_size("tp")
    chips = minor // CORES
    assert specialist_switch_matrix.shape[0] == CORES
    experts = CORES * peers
    capacity = max(2, 3 * TOP * rows // (2 * experts))
    room = -(-capacity // 8) * 8

    def to_partner(value):
        return lax.ppermute(value, "tp", [(t, t ^ 1) for t in range(minor)])

    def to_chip(value, ahead):
        pairs = [(t, (t + CORES * ahead) % minor) for t in range(minor)]
        return lax.ppermute(value, "tp", pairs)

    def to_peer(value, o):
        pairs = [
            (s * minor + t, (s ^ (o // CORES)) * minor + (t ^ (o % CORES)))
            for s in range(peers)
            for t in range(minor)
        ]
        return lax.ppermute(value, ("sp", "tp"), pairs)

    piece = jax.ShapeDtypeStruct((rows, width), BF16)
    widths = chunk_widths(width)
    slim = [jax.ShapeDtypeStruct((rows, columns), BF16) for columns in widths]

    def early(*inputs):
        small = (raw_increments, channel_log_fade_speed, extra_log_fade)
        return kernel(
            early_kernel,
            (*small, *inputs),
            [jax.ShapeDtypeStruct(v.shape, v.dtype) for v in inputs]
            + [
                jax.ShapeDtypeStruct(raw_increments.shape, F32),
                jax.ShapeDtypeStruct((raw_increments.shape[2], STATE), F32),
                jax.ShapeDtypeStruct((*raw_increments.shape[:2], STATE), F32),
            ],
            in_specs=[pl.BlockSpec(memory_space=pltpu.HBM)] * (len(small) + len(inputs)),
            scratch_shapes=[pltpu.VMEM(v.shape, v.dtype) for v in small]
            + [pltpu.SemaphoreType.DMA((len(small) + len(inputs),))],
        )

    keep, send = mixer(
        channel_feed_mapped,
        write_coefficient_mapped,
        emission_coefficient_mapped,
        channel_feed_taps,
        write_coefficient_taps,
        emission_coefficient_taps,
        early,
        result_switch_mapped,
        cluster_scaling_factor,
        rows,
    )
    own = (specialist_switch_matrix, specialist_widen_matrix, specialist_contract_matrix)
    other = tuple(to_partner(value) for value in own)
    parts = kernel(
        project_kernel,
        (keep, to_partner(send), blend_result_matrix, to_partner(blend_result_matrix)),
        [piece] * chips,
    )
    parts = [parts[0]] + [to_chip(parts[r], r) for r in range(1, chips)]
    after, *normed = kernel(
        functools.partial(after_kernel, chips=chips),
        (skip_stream_entry, routing_scaling_factor.reshape(1, -1), *parts),
        [piece] + slim,
    )
    meta = kernel(
        functools.partial(route_kernel, room=room),
        (picked_specialists, router_affinities),
        jax.ShapeDtypeStruct((rows, TILE), F32),
    )
    metas = [meta] + [to_chip(meta, r) for r in range(1, chips)]
    places = dict(chips=chips, room=room, axis="sp", minor="tp")
    few = jax.ShapeDtypeStruct((room, widths[-1]), BF16)
    stack = jax.ShapeDtypeStruct((experts * room, widths[-1]), BF16)
    message = jax.ShapeDtypeStruct((chips * room, widths[-1]), BF16)
    sends = kernel(
        functools.partial(dispatch_kernel, **{**places, "chips": 1}),
        (meta, normed[-1]),
        [few] * experts,
    )
    sends = [sends[0]] + [to_peer(sends[o], o) for o in range(1, experts)]
    (stacked,) = kernel(functools.partial(regroup_kernel, count=experts, parts=1), sends, [stack])
    stacked = [stacked] + [to_chip(stacked, r) for r in range(1, chips)]
    last = kernel(
        functools.partial(regroup_kernel, count=chips, parts=experts), stacked, [message] * experts
    )

    messages = []
    for n in range(CHUNKS):
        message = jax.ShapeDtypeStruct((chips * room, widths[n]), BF16)
        tokens = [normed[n]] + [to_chip(normed[n], r) for r in range(1, chips)]
        sends = kernel(
            functools.partial(dispatch_kernel, **places), (*metas, *tokens), [message] * experts
        )
        messages.append([sends[0]] + [to_peer(sends[o], o) for o in range(1, experts)])
    messages.append(last)
    gate, up, down = side_by_side(own, other)
    bounds = group_bounds(peers)
    results = [[] for _ in widths]
    for first, end in zip(bounds[:-1], bounds[1:]):
        part = [[chunk[o] for chunk in messages] for o in range(first, end)]
        done = run_experts(part, gate, up, down)
        for chunk, more in zip(results, done):
            chunk += more
    shares = kernel(
        functools.partial(regroup_kernel, count=experts, parts=chips), results[-1], [stack] * chips
    )
    shares = [shares[0]] + [to_chip(shares[chips - r], r) for r in range(1, chips)]
    sends = kernel(functools.partial(spread_kernel, count=chips), shares, [few] * experts)
    back = [sends[0]] + [to_peer(sends[o], o) for o in range(1, experts)]
    last = kernel(
        functools.partial(own_combine_kernel, room=room, axis="sp", minor="tp"),
        (meta, *back),
        slim[-1],
    )
    pieces = []
    for n in range(CHUNKS):
        back = [results[n][0]] + [to_peer(results[n][o], o) for o in range(1, experts)]
        sums = kernel(
            functools.partial(combine_kernel, **places), (*metas, *back), [slim[n]] * chips
        )
        pieces += [sums[0]] + [to_chip(sums[chips - r], r) for r in range(1, chips)]
    return kernel(
        functools.partial(final_kernel, counts=(chips,) * CHUNKS + (1,)),
        (after, *pieces, last),
        piece,
    )


def group_bounds(peers):
    return [0, CORES, CORES * (peers // 2 + 1), CORES * peers]


def solution(mesh):
    in_specs = (
        P(("sp", "tp"), None),
        P("sp", "tp"),
        P("sp", "tp"),
        P("sp", "tp"),
        P("sp", "tp"),
        P(None, "tp"),
        P(None, "tp"),
        P(None, "tp"),
        P(None, "tp", "sp"),
        P(None, "tp"),
        P(None, "tp", "sp"),
        P("tp"),
        P("tp", None),
        P(),
        P("sp", None, "tp"),
        P("sp", None, "tp"),
        P("sp", "tp", None),
        P(("sp", "tp"), None),
        P(("sp", "tp"), None),
    )
    out_specs = P(("sp", "tp"), None)

    return jax.shard_map(
        per_device, mesh=mesh, in_specs=in_specs, out_specs=out_specs, check_vma=False
    )
```

```python
import functools
import math

import jax
import jax.numpy as jnp
from jax import lax
from jax.experimental import pallas as pl
from jax.experimental.pallas import tpu as pltpu
from jax.sharding import PartitionSpec as P


HEAD_DIM = 64
STATE = 128
TOP = 2
TILE = 128
PAD = 8
SPREAD = 2
EXTRA = 16

EPSILON = 1e-06
LOG2E = math.log2(math.e)
F32, BF16 = jnp.float32, jnp.bfloat16


CORES = 2
CHUNKS = 2


def chunk_widths(width):
    last = max(width // 8 // (2 * TILE), 1) * 2 * TILE * SPREAD
    second = (width - last) // 2 // (2 * TILE) * 2 * TILE
    return (width - last - second, second, last)


def chip_and_core(axis):
    at = lax.axis_index(axis)
    return at // CORES, at & (CORES - 1)


def silu(v):
    return v / (1.0 + jnp.exp(-v))


def over_heads(columns, first, count):
    rows = columns.shape[0]
    lane = lax.broadcasted_iota(jnp.int32, (rows, 2 * HEAD_DIM), 1)
    pairs = []
    for h in range(0, count, 2):
        a = jnp.broadcast_to(columns[:, first + h : first + h + 1], lane.shape)
        b = jnp.broadcast_to(columns[:, first + h + 1 : first + h + 2], lane.shape)
        pairs.append(jnp.where(lane < HEAD_DIM, a, b))
    return jnp.concatenate(pairs, axis=1)


def route_kernel(picked_ref, affinity_ref, meta_ref, *, room):
    rows = picked_ref.shape[0]
    lane = lax.broadcasted_iota(jnp.int32, (rows, TILE), 1)
    picks = [jnp.broadcast_to(picked_ref[:, k : k + 1], (rows, TILE)) == lane for k in range(TOP)]
    member = jnp.where(picks[0] | picks[1], 1.0, 0.0)
    earlier = lax.broadcasted_iota(jnp.int32, (rows, rows), 0) > lax.broadcasted_iota(
        jnp.int32, (rows, rows), 1
    )
    rank = jnp.dot(
        jnp.where(earlier, 1.0, 0.0).astype(BF16), member.astype(BF16), preferred_element_type=F32
    )
    affinity = affinity_ref[...]
    total = jnp.sum(affinity, axis=1, keepdims=True)
    meta = jnp.zeros((rows, TILE), F32)
    for k in range(TOP):
        slot = picked_ref[:, k : k + 1].astype(F32) * room + jnp.sum(
            jnp.where(picks[k], rank, 0.0), axis=1, keepdims=True
        )
        meta = jnp.where(lane == k, slot, meta)
        meta = jnp.where(lane == TOP + k, affinity[:, k : k + 1] / total, meta)
    meta_ref[...] = meta


def early_kernel(step_ref, decay_ref, rows_ref, cols_ref, totals_ref):
    heads, steps = step_ref.shape[1:]
    lane = lax.broadcasted_iota(jnp.int32, (heads, steps), 1)
    sums, weights = [], []
    for d in range(2):
        step, run = step_ref[d], decay_ref[d]
        shift = 1
        while shift < steps:
            if d == 0:
                run = run + jnp.where(lane >= shift, pltpu.roll(run, shift, 1), 0.0)
            else:
                run = run + jnp.where(lane < steps - shift, pltpu.roll(run, steps - shift, 1), 0.0)
            shift *= 2
        total = run[:, steps - 1 : steps] if d == 0 else run[:, 0:1]
        totals_ref[d] = jnp.broadcast_to(total, (heads, STATE))
        sums.append(run * LOG2E)
        weights.append(jnp.exp(total - run) * step)
        rows_ref[d] = run * LOG2E - jnp.log(step) * LOG2E
    stacked = jnp.concatenate(
        sums + weights + [jnp.zeros((STATE - 4 * heads, steps), F32)], axis=0
    )
    cols_ref[...] = stacked.T


def prepare_kernel(
    all_ref, low_ref, high_ref, taps_ref, cols_ref, totals_ref,
    xc_ref, bc_ref, cc_ref, *rest, axis,
):
    *msg_refs, pad_ref = rest
    steps = all_ref.shape[0]
    heads = totals_ref.shape[1]
    groups = bc_ref.shape[1] // STATE
    per_group = heads // groups
    wide = per_group * HEAD_DIM
    here = lax.axis_index(axis)
    cols = cols_ref[...]
    totals = [totals_ref[d, :, 0:1] for d in range(2)]

    def conv(start):
        lanes = slice(start, start + TILE)
        pad_ref[PAD - 2 : PAD] = low_ref[:, lanes].astype(F32)
        pad_ref[PAD : PAD + steps] = all_ref[:, lanes].astype(F32)
        pad_ref[PAD + steps : PAD + steps + 2] = high_ref[:, lanes].astype(F32)
        taps = taps_ref[:, lanes].astype(F32)
        total = taps[0:1] * pad_ref[PAD - 2 : PAD - 2 + steps]
        for j in range(1, taps.shape[0]):
            total = total + taps[j : j + 1] * pad_ref[PAD - 2 + j : PAD - 2 + j + steps]
        return silu(total)

    at = 0
    for out_ref in (xc_ref, bc_ref, cc_ref):
        for start in range(0, out_ref.shape[1], TILE):
            out_ref[:, start : start + TILE] = conv(at + start).astype(BF16)
        at += out_ref.shape[1]

    row = lax.broadcasted_iota(jnp.int32, (EXTRA, wide), 0)
    own = lax.broadcasted_iota(jnp.int32, (per_group, wide), 0) == (
        lax.broadcasted_iota(jnp.int32, (per_group, wide), 1) // HEAD_DIM
    )
    for g in range(groups):
        turned = bc_ref[:, g * STATE : (g + 1) * STATE].astype(F32).T.astype(BF16)
        xg = xc_ref[:, g * wide : (g + 1) * wide].astype(F32)
        both = []
        for d in range(2):
            weight = over_heads(cols, (2 + d) * heads + g * per_group, per_group)
            state = jnp.dot(turned, (xg * weight).astype(BF16), preferred_element_type=F32)
            total = jnp.sum(
                jnp.where(own, totals[d][g * per_group : (g + 1) * per_group], 0.0),
                axis=0, keepdims=True,
            )
            upper = total.astype(BF16).astype(F32)
            extra = jnp.where(row == 0, upper, jnp.where(row == 1, total - upper, 0.0))
            both.append((state, extra))
        for k, msg_ref in enumerate(msg_refs, 1):
            onward = jnp.where((here ^ k) > here, 1.0, 0.0).astype(F32)
            (sf, ef), (sb, eb) = both
            msg_ref[g, 0:STATE, :] = (sf * onward + sb * (1.0 - onward)).astype(BF16)
            msg_ref[g, STATE : STATE + EXTRA, :] = (ef * onward + eb * (1.0 - onward)).astype(BF16)


def local_kernel(xc_ref, bc_ref, cc_ref, rows_ref, cols_ref, y_ref):
    steps = xc_ref.shape[0]
    heads = rows_ref.shape[1]
    groups = bc_ref.shape[1] // STATE
    per_group = heads // groups
    tiles = steps // TILE
    i_at = lax.broadcasted_iota(jnp.int32, (TILE, TILE), 0)
    j_at = lax.broadcasted_iota(jnp.int32, (TILE, TILE), 1)
    for g in range(groups):
        for i in range(tiles):
            span = slice(i * TILE, (i + 1) * TILE)
            inner = lax.dot_general(
                cc_ref[span, g * STATE : (g + 1) * STATE],
                bc_ref[:, g * STATE : (g + 1) * STATE],
                (((1,), (1,)), ((), ())),
                preferred_element_type=F32,
            )
            for pair in range(per_group // 2):
                halves = []
                at = (g * per_group + 2 * pair) * HEAD_DIM
                for h in (g * per_group + 2 * pair, g * per_group + 2 * pair + 1):
                    here_f = jnp.broadcast_to(cols_ref[span, h : h + 1], (TILE, TILE))
                    here_b = jnp.broadcast_to(cols_ref[span, heads + h : heads + h + 1], (TILE, TILE))
                    parts = []
                    for j in range(tiles):
                        js = slice(j * TILE, (j + 1) * TILE)
                        if j <= i:
                            mix = jnp.exp2(here_f - rows_ref[0, h : h + 1, js])
                            if j == i:
                                mix = jnp.where(i_at >= j_at, mix, 0.0) + jnp.where(
                                    i_at <= j_at, jnp.exp2(here_b - rows_ref[1, h : h + 1, js]), 0.0
                                )
                        else:
                            mix = jnp.exp2(here_b - rows_ref[1, h : h + 1, js])
                        parts.append((mix * inner[:, js]).astype(BF16))
                    halves.append(
                        jnp.dot(
                            jnp.concatenate(parts, axis=1),
                            xc_ref[:, at : at + 2 * HEAD_DIM],
                            preferred_element_type=F32,
                        )
                    )
                y_ref[span, at : at + 2 * HEAD_DIM] = jnp.where(j_at < HEAD_DIM, *halves)


def finish_kernel(y_ref, cc_ref, cols_ref, switch_ref, gain_ref, *rest, axis, minor, rows):
    *msg_refs, keep_ref, send_ref, carry_ref = rest
    steps, channels = y_ref.shape
    groups = cc_ref.shape[1] // STATE
    wide = channels // groups
    per_group = wide // HEAD_DIM
    heads = groups * per_group
    here = lax.axis_index(axis)
    chip, core = chip_and_core(minor)
    chips = lax.axis_size(minor) // CORES
    peers = [here ^ k for k in range(1, len(msg_refs) + 1)]

    def flag(condition):
        return jnp.where(condition, 1.0, 0.0).astype(F32)

    for g in range(groups):
        totals = [
            ref[g, STATE : STATE + 1, :].astype(F32) + ref[g, STATE + 1 : STATE + 2, :].astype(F32)
            for ref in msg_refs
        ]
        for d in range(2):
            carry = jnp.zeros((STATE, wide), F32)
            for k, ref in enumerate(msg_refs):
                between = jnp.zeros((1, wide), F32)
                for other in range(len(msg_refs)):
                    if other != k:
                        if d == 0:
                            inside = (peers[k] < peers[other]) & (peers[other] < here)
                        else:
                            inside = (peers[k] > peers[other]) & (peers[other] > here)
                        between = between + flag(inside) * totals[other]
                mine = flag(peers[k] < here if d == 0 else peers[k] > here)
                carry = carry + ref[g, 0:STATE, :].astype(F32) * (mine * jnp.exp(between))
            carry_ref[d] = carry.astype(BF16)
        for i in range(steps // TILE):
            span = slice(i * TILE, (i + 1) * TILE)
            lanes = slice(g * wide, (g + 1) * wide)
            cols = jnp.exp2(cols_ref[span, :])
            cc = cc_ref[span, g * STATE : (g + 1) * STATE]
            y = y_ref[span, lanes]
            for d in range(2):
                y = y + over_heads(cols, d * heads + g * per_group, per_group) * jnp.dot(
                    cc, carry_ref[d], preferred_element_type=F32
                )
            gated = y * silu(switch_ref[span, lanes].astype(F32))
            mean = jnp.sum(gated * gated, axis=1, keepdims=True) * (1.0 / wide)
            mixed = gated * lax.rsqrt(mean + EPSILON) * gain_ref[:, lanes]
            for part in range(TILE // (CORES * rows)):
                block = i * (TILE // (CORES * rows)) + part
                south = mixed[part * CORES * rows : (part * CORES + 1) * rows]
                north = mixed[(part * CORES + 1) * rows : (part + 1) * CORES * rows]
                odd = flag(core == 1)
                at = pl.multiple_of(((block - chip) & (chips - 1)) * rows, rows)
                keep_ref[pl.ds(at, rows), lanes] = (south * (1.0 - odd) + north * odd).astype(BF16)
                send_ref[pl.ds(at, rows), lanes] = (south * odd + north * (1.0 - odd)).astype(BF16)


def kernel(body, operands, outs, grant=12, **settings):
    return pl.pallas_call(
        body,
        out_shape=outs,
        out_specs=vmem(len(outs)) if isinstance(outs, list) else vmem(1)[0],
        compiler_params=pltpu.CompilerParams(vmem_limit_bytes=grant * 1024 * 1024),
        **({} if "in_specs" in settings else dict(in_specs=vmem(len(operands)))),
        **settings,
    )(*operands)


def vmem(count):
    return [pl.BlockSpec(memory_space=pltpu.VMEM) for _ in range(count)]


def mixer(x, b, c, tx, tb, tc, early, switch, gain, block_rows):
    steps, channels = x.shape
    groups = b.shape[1] // STATE
    wide = channels // groups
    rim = tx.shape[0] // 2
    count = lax.axis_size("sp")
    first = jnp.concatenate([x[:rim], b[:rim], c[:rim]], axis=1)
    last = jnp.concatenate([x[-rim:], b[-rim:], c[-rim:]], axis=1)
    low = lax.ppermute(last, "sp", [(i, i + 1) for i in range(count - 1)])
    high = lax.ppermute(first, "sp", [(i + 1, i) for i in range(count - 1)])
    rows, cols, totals = early()
    heads = rows.shape[1]
    message = jax.ShapeDtypeStruct((groups, STATE + EXTRA, wide), BF16)
    xc, bc, cc, *sends = kernel(
        functools.partial(prepare_kernel, axis="sp"),
        (
            jnp.concatenate([x, b, c], axis=1),
            low,
            high,
            jnp.concatenate([tx, tb, tc], axis=1),
            cols,
            totals,
        ),
        [jax.ShapeDtypeStruct(v.shape, BF16) for v in (x, b, c)] + [message] * (count - 1),
        scratch_shapes=[pltpu.VMEM((steps + 2 * PAD, TILE), F32)],
    )
    arrived = [
        lax.ppermute(send, "sp", [(i, i ^ k) for i in range(count)])
        for k, send in enumerate(sends, 1)
    ]
    y = kernel(
        local_kernel,
        (xc, bc, cc, rows, cols),
        jax.ShapeDtypeStruct(x.shape, F32),
        cost_estimate=pl.CostEstimate(
            flops=2 * steps * steps * (channels + groups * STATE) * 4,
            bytes_accessed=8 * steps * channels,
            transcendentals=heads * steps * steps,
        ),
    )
    return kernel(
        functools.partial(finish_kernel, axis="sp", minor="tp", rows=block_rows),
        (y, cc, cols, switch, gain.reshape(1, -1), *arrived),
        [jax.ShapeDtypeStruct((steps // CORES, channels), BF16)] * 2,
        scratch_shapes=[pltpu.VMEM((2, STATE, wide), BF16)],
    )


def project_kernel(keep_ref, other_ref, own_w_ref, other_w_ref, *out_refs):
    rows = out_refs[0].shape[0]
    width = own_w_ref.shape[1]
    step = 2 * TILE
    for n in range(0, width, step):
        lanes = slice(n, n + step)
        part = jnp.dot(keep_ref[...], own_w_ref[:, lanes], preferred_element_type=F32) + jnp.dot(
            other_ref[...], other_w_ref[:, lanes], preferred_element_type=F32
        )
        for r, out_ref in enumerate(out_refs):
            out_ref[:, lanes] = part[r * rows : (r + 1) * rows].astype(BF16)


def after_kernel(skip_ref, gain_ref, *refs, chips):
    part_refs, (after_ref, *normed_refs) = refs[:chips], refs[chips:]
    total = skip_ref[...].astype(F32)
    for ref in part_refs:
        total = total + ref[...].astype(F32)
    after = total.astype(BF16)
    after_ref[...] = after
    values = after.astype(F32)
    mean = jnp.sum(values * values, axis=1, keepdims=True) * (1.0 / values.shape[1])
    normed = (values * lax.rsqrt(mean + EPSILON) * gain_ref[...]).astype(BF16)
    at = 0
    for ref in normed_refs:
        ref[...] = normed[:, at : at + ref.shape[1]]
        at += ref.shape[1]


def final_kernel(after_ref, *refs, counts):
    *in_refs, out_ref = refs
    at = 0
    for count in counts:
        part_refs, in_refs = in_refs[:count], in_refs[count:]
        lanes = slice(at, at + part_refs[0].shape[1])
        total = after_ref[:, lanes].astype(F32)
        for ref in part_refs:
            total = total + ref[...].astype(F32)
        out_ref[:, lanes] = total.astype(BF16)
        at = lanes.stop


def regroup_kernel(*refs, count, parts):
    in_refs, out_refs = refs[:count], refs[count:]
    rows = in_refs[0].shape[0] // parts
    values = [ref[...].astype(F32) for ref in in_refs]
    for n, ref in enumerate(out_refs):
        span = slice(n * rows, (n + 1) * rows)
        ref[...] = jnp.concatenate([value[span] for value in values], axis=0).astype(BF16)


def spread_kernel(*refs, count):
    total = refs[0][...].astype(F32)
    for ref in refs[1:count]:
        total = total + ref[...].astype(F32)
    for n, ref in enumerate(refs[count:]):
        rows = ref.shape[0]
        ref[...] = total[n * rows : (n + 1) * rows].astype(BF16)


def own_combine_kernel(meta_ref, *refs, room, axis, minor):
    *in_refs, out_ref = refs
    rows = out_ref.shape[0]
    here = lax.axis_index(axis)
    core = chip_and_core(minor)[1]
    meta = meta_ref[...]
    lane = lax.broadcasted_iota(jnp.int32, (rows, len(in_refs) * room), 1)
    slot = lane
    for o in range(len(in_refs)):
        expert = (here ^ (o // CORES)) * CORES + (core ^ (o % CORES))
        inside = (lane >= o * room) & (lane < (o + 1) * room)
        slot = jnp.where(inside, lane + (expert - o) * room, slot)
    slot = slot.astype(F32)
    weight = jnp.where(meta[:, 0:1] == slot, meta[:, TOP : TOP + 1], 0.0) + jnp.where(
        meta[:, 1:2] == slot, meta[:, TOP + 1 : TOP + 2], 0.0
    )
    values = jnp.concatenate([ref[...].astype(F32) for ref in in_refs], axis=0).astype(BF16)
    out_ref[...] = jnp.dot(
        weight.astype(BF16), values, preferred_element_type=F32
    ).astype(BF16)


def dispatch_kernel(*refs, chips, room, axis, minor):
    meta_refs, x_refs, out_refs = refs[:chips], refs[chips : 2 * chips], refs[2 * chips :]
    rows, width = x_refs[0].shape
    here = lax.axis_index(axis)
    core = chip_and_core(minor)[1]
    lanes_used = max(chips * rows, TILE)
    spare = lanes_used - chips * rows
    metas = [ref[...] for ref in meta_refs]
    if spare:
        metas.append(jnp.zeros((spare, TILE), F32))
    meta = jnp.concatenate(metas, axis=0).T
    rank = lax.broadcasted_iota(jnp.int32, (room, lanes_used), 0).astype(F32)
    source = lax.broadcasted_iota(jnp.int32, (room, lanes_used), 1) // rows
    chosen = []
    for o in range(len(out_refs)):
        expert = (here ^ (o // CORES)) * CORES + (core ^ (o % CORES))
        first = (expert * room).astype(F32)
        hit = (meta[0:1] - first == rank) | (meta[1:2] - first == rank)
        chosen += [
            jnp.where(hit & (source == r), 1.0, 0.0).astype(F32) for r in range(chips)
        ]
    chosen = jnp.concatenate(chosen, axis=0).astype(BF16)
    for n in range(0, width, 2 * TILE):
        lanes = slice(n, n + 2 * TILE)
        tokens = [ref[:, lanes] for ref in x_refs]
        if spare:
            tokens.append(jnp.zeros((spare, 2 * TILE), BF16))
        tokens = jnp.concatenate(tokens, axis=0)
        out = jnp.dot(chosen, tokens, preferred_element_type=F32)
        for o, ref in enumerate(out_refs):
            ref[:, lanes] = out[o * chips * room : (o + 1) * chips * room].astype(BF16)


def combine_kernel(*refs, chips, room, axis, minor):
    meta_refs, in_refs, out_refs = refs[:chips], refs[chips:-chips], refs[-chips:]
    rows, width = out_refs[0].shape
    here = lax.axis_index(axis)
    core = chip_and_core(minor)[1]
    lane = lax.broadcasted_iota(jnp.int32, (rows, chips * room), 1)
    weights = []
    for r in range(chips):
        meta = meta_refs[r][...]
        parts = []
        for o in range(len(in_refs)):
            expert = (here ^ (o // CORES)) * CORES + (core ^ (o % CORES))
            slot = (lane - r * room + expert * room).astype(F32)
            inside = (lane >= r * room) & (lane < (r + 1) * room)
            both = jnp.where(meta[:, 0:1] == slot, meta[:, TOP : TOP + 1], 0.0) + jnp.where(
                meta[:, 1:2] == slot, meta[:, TOP + 1 : TOP + 2], 0.0
            )
            parts.append(jnp.where(inside, both, 0.0).astype(BF16))
        weights.append(parts)
    for n in range(0, width, 2 * TILE):
        lanes = slice(n, n + 2 * TILE)
        total = jnp.zeros((chips * rows, 2 * TILE), F32)
        for o, ref in enumerate(in_refs):
            weight = jnp.concatenate([weights[r][o] for r in range(chips)], axis=0)
            total = total + jnp.dot(weight, ref[:, lanes], preferred_element_type=F32)
        for r, ref in enumerate(out_refs):
            ref[:, lanes] = total[r * rows : (r + 1) * rows].astype(BF16)


def weights_kernel(*refs, minor):
    in_refs, (gate_ref, up_ref, down_ref, sems) = refs[:6], refs[6:]
    core = chip_and_core(minor)[1]
    slabs, _, step = gate_ref.shape
    per_source = slabs // 2
    half = down_ref.shape[0] // 2
    copies = []
    for side in range(2):
        gate, up, down = in_refs[3 * side : 3 * side + 3]
        for t in range(per_source):
            at, span = side * per_source + t, pl.ds(t * step, step)
            copies.append((gate.at[core, :, span], gate_ref.at[at]))
            copies.append((up.at[core, :, span], up_ref.at[at]))
        copies.append((down.at[core], down_ref.at[pl.ds(side * half, half)]))
    copies = [pltpu.make_async_copy(a, b, sems.at[n]) for n, (a, b) in enumerate(copies)]
    for copy in copies:
        copy.start()
    for copy in copies:
        copy.wait()


def hidden_kernel(*refs, count, chunks):
    x_refs, (gate_ref, up_ref, hidden_ref, x_vmem) = refs[:count], refs[count:]
    slabs, _, step = gate_ref.shape
    rows, at = x_refs[0].shape[0], 0
    for n in range(chunks):
        columns = x_refs[n].shape[1]
        for o, ref in enumerate(x_refs[n::chunks]):
            x_vmem[o * rows : (o + 1) * rows, at : at + columns] = ref[...]
        at += columns
    for t in range(slabs):
        gate = jnp.dot(x_vmem[...], gate_ref[t], preferred_element_type=F32)
        up = jnp.dot(x_vmem[...], up_ref[t], preferred_element_type=F32)
        hidden_ref[:, t * step : (t + 1) * step] = (silu(gate) * up).astype(BF16)


def down_kernel(hidden_ref, down_ref, *out_refs, first):
    rows, columns = out_refs[0].shape
    for n in range(0, columns, 2 * TILE):
        at = first + n
        part = jnp.dot(
            hidden_ref[...], down_ref[:, at : at + 2 * TILE], preferred_element_type=F32
        ).astype(BF16)
        for o, ref in enumerate(out_refs):
            ref[:, n : n + 2 * TILE] = part[o * rows : (o + 1) * rows]


def side_by_side(own, other):
    _, width, hidden = own[0].shape
    step = 2 * TILE if hidden % (2 * TILE) == 0 else hidden
    slabs = 2 * (hidden // step)
    return kernel(
        functools.partial(weights_kernel, minor="tp"),
        (*own, *other),
        [jax.ShapeDtypeStruct((slabs, width, step), BF16)] * 2
        + [jax.ShapeDtypeStruct((2 * hidden, width), BF16)],
        grant=28,
        in_specs=[pl.BlockSpec(memory_space=pltpu.HBM)] * 6,
        scratch_shapes=[pltpu.SemaphoreType.DMA((2 * slabs + 2,))],
    )


def run_experts(messages, gate, up, down):
    flat = [part for message in messages for part in message]
    widths = [part.shape[1] for part in messages[0]]
    rows, width = flat[0].shape[0], sum(widths)
    total_rows, hidden = len(messages) * rows, down.shape[0]
    inner = kernel(
        functools.partial(hidden_kernel, count=len(flat), chunks=len(widths)),
        (*flat, gate, up),
        jax.ShapeDtypeStruct((total_rows, hidden), BF16),
        grant=24,
        scratch_shapes=[pltpu.VMEM((total_rows, width), BF16)],
        cost_estimate=pl.CostEstimate(
            flops=4 * total_rows * width * hidden,
            bytes_accessed=4 * hidden * width,
            transcendentals=total_rows * hidden,
        ),
    )
    return [
        kernel(
            functools.partial(down_kernel, first=sum(widths[:n])),
            (inner, down),
            [jax.ShapeDtypeStruct((rows, columns), BF16)] * len(messages),
            cost_estimate=pl.CostEstimate(
                flops=2 * total_rows * columns * hidden,
                bytes_accessed=2 * hidden * columns,
                transcendentals=0,
            ),
        )
        for n, columns in enumerate(widths)
    ]


def per_device(
    skip_stream_entry,
    result_switch_mapped,
    channel_feed_mapped,
    write_coefficient_mapped,
    emission_coefficient_mapped,
    channel_feed_taps,
    write_coefficient_taps,
    emission_coefficient_taps,
    raw_increments,
    channel_log_fade_speed,
    extra_log_fade,
    cluster_scaling_factor,
    blend_result_matrix,
    routing_scaling_factor,
    specialist_switch_matrix,
    specialist_widen_matrix,
    specialist_contract_matrix,
    picked_specialists,
    router_affinities,
):
    rows, width = skip_stream_entry.shape
    peers, minor = lax.axis_size("sp"), lax.axis_size("tp")
    chips = minor // CORES
    assert specialist_switch_matrix.shape[0] == CORES
    experts = CORES * peers
    capacity = max(2, 3 * TOP * rows // (2 * experts))
    room = -(-capacity // 8) * 8

    def to_partner(value):
        return lax.ppermute(value, "tp", [(t, t ^ 1) for t in range(minor)])

    def to_chip(value, ahead):
        pairs = [(t, (t + CORES * ahead) % minor) for t in range(minor)]
        return lax.ppermute(value, "tp", pairs)

    def to_peer(value, o):
        pairs = [
            (s * minor + t, (s ^ (o // CORES)) * minor + (t ^ (o % CORES)))
            for s in range(peers)
            for t in range(minor)
        ]
        return lax.ppermute(value, ("sp", "tp"), pairs)

    piece = jax.ShapeDtypeStruct((rows, width), BF16)
    widths = chunk_widths(width)
    slim = [jax.ShapeDtypeStruct((rows, columns), BF16) for columns in widths]

    def early():
        step = jax.nn.softplus(raw_increments.astype(F32))
        decay = extra_log_fade - step * jnp.exp(channel_log_fade_speed)[..., None]
        return kernel(
            early_kernel,
            (step, decay),
            [
                jax.ShapeDtypeStruct(raw_increments.shape, F32),
                jax.ShapeDtypeStruct((raw_increments.shape[2], STATE), F32),
                jax.ShapeDtypeStruct((*raw_increments.shape[:2], STATE), F32),
            ],
        )

    keep, send = mixer(
        channel_feed_mapped,
        write_coefficient_mapped,
        emission_coefficient_mapped,
        channel_feed_taps,
        write_coefficient_taps,
        emission_coefficient_taps,
        early,
        result_switch_mapped,
        cluster_scaling_factor,
        rows,
    )
    own = (specialist_switch_matrix, specialist_widen_matrix, specialist_contract_matrix)
    other = tuple(to_partner(value) for value in own)
    parts = kernel(
        project_kernel,
        (keep, to_partner(send), blend_result_matrix, to_partner(blend_result_matrix)),
        [piece] * chips,
    )
    parts = [parts[0]] + [to_chip(parts[r], r) for r in range(1, chips)]
    after, *normed = kernel(
        functools.partial(after_kernel, chips=chips),
        (skip_stream_entry, routing_scaling_factor.reshape(1, -1), *parts),
        [piece] + slim,
    )
    meta = kernel(
        functools.partial(route_kernel, room=room),
        (picked_specialists, router_affinities),
        jax.ShapeDtypeStruct((rows, TILE), F32),
    )
    metas = [meta] + [to_chip(meta, r) for r in range(1, chips)]
    places = dict(chips=chips, room=room, axis="sp", minor="tp")
    few = jax.ShapeDtypeStruct((room, widths[-1]), BF16)
    stack = jax.ShapeDtypeStruct((experts * room, widths[-1]), BF16)
    message = jax.ShapeDtypeStruct((chips * room, widths[-1]), BF16)
    sends = kernel(
        functools.partial(dispatch_kernel, **{**places, "chips": 1}),
        (meta, normed[-1]),
        [few] * experts,
    )
    sends = [sends[0]] + [to_peer(sends[o], o) for o in range(1, experts)]
    (stacked,) = kernel(functools.partial(regroup_kernel, count=experts, parts=1), sends, [stack])
    stacked = [stacked] + [to_chip(stacked, r) for r in range(1, chips)]
    last = kernel(
        functools.partial(regroup_kernel, count=chips, parts=experts), stacked, [message] * experts
    )

    messages = []
    for n in range(CHUNKS):
        message = jax.ShapeDtypeStruct((chips * room, widths[n]), BF16)
        tokens = [normed[n]] + [to_chip(normed[n], r) for r in range(1, chips)]
        sends = kernel(
            functools.partial(dispatch_kernel, **places), (*metas, *tokens), [message] * experts
        )
        messages.append([sends[0]] + [to_peer(sends[o], o) for o in range(1, experts)])
    messages.append(last)
    gate, up, down = side_by_side(own, other)
    bounds = group_bounds(peers)
    results = [[] for _ in widths]
    for first, end in zip(bounds[:-1], bounds[1:]):
        part = [[chunk[o] for chunk in messages] for o in range(first, end)]
        done = run_experts(part, gate, up, down)
        for chunk, more in zip(results, done):
            chunk += more
    shares = kernel(
        functools.partial(regroup_kernel, count=experts, parts=chips), results[-1], [stack] * chips
    )
    shares = [shares[0]] + [to_chip(shares[chips - r], r) for r in range(1, chips)]
    sends = kernel(functools.partial(spread_kernel, count=chips), shares, [few] * experts)
    back = [sends[0]] + [to_peer(sends[o], o) for o in range(1, experts)]
    last = kernel(
        functools.partial(own_combine_kernel, room=room, axis="sp", minor="tp"),
        (meta, *back),
        slim[-1],
    )
    pieces = []
    for n in range(CHUNKS):
        back = [results[n][0]] + [to_peer(results[n][o], o) for o in range(1, experts)]
        sums = kernel(
            functools.partial(combine_kernel, **places), (*metas, *back), [slim[n]] * chips
        )
        pieces += [sums[0]] + [to_chip(sums[chips - r], r) for r in range(1, chips)]
    return kernel(
        functools.partial(final_kernel, counts=(chips,) * CHUNKS + (1,)),
        (after, *pieces, last),
        piece,
    )


def group_bounds(peers):
    return [0, CORES, CORES * (peers // 2 + 1), CORES * peers]


def solution(mesh):
    in_specs = (
        P(("sp", "tp"), None),
        P("sp", "tp"),
        P("sp", "tp"),
        P("sp", "tp"),
        P("sp", "tp"),
        P(None, "tp"),
        P(None, "tp"),
        P(None, "tp"),
        P(None, "tp", "sp"),
        P(None, "tp"),
        P(None, "tp", "sp"),
        P("tp"),
        P("tp", None),
        P(),
        P("sp", None, "tp"),
        P("sp", None, "tp"),
        P("sp", "tp", None),
        P(("sp", "tp"), None),
        P(("sp", "tp"), None),
    )
    out_specs = P(("sp", "tp"), None)

    return jax.shard_map(
        per_device, mesh=mesh, in_specs=in_specs, out_specs=out_specs, check_vma=False
    )
```
